128 devices in a mesh: sp: 16 (over z, x), dp: 8 (over y, core).
Axes of the slice: x: 4, y: 4, z: 4, core: 2. Of those that a mesh axis runs over, the one named last changes fastest.
Arguments:
- queries: bfloat16 [8, 2048, 2048], P('dp', 'sp'), may hold values from -9 to 9
- keys: bfloat16 [8, 2048, 512], P('dp', 'sp'), may hold values from -9 to 9
- values: bfloat16 [8, 2048, 512], P('dp', 'sp'), may hold values from -6 to 6
- out_grad: bfloat16 [8, 2048, 2048], P('dp', 'sp'), may hold values from -24 to 24
- layer_in: bfloat16 [8, 2048, 4096], P('dp', 'sp'), may hold values from -0.09375 to 0.09375
- key_weight: bfloat16 [4096, 512], P('dp'), may hold values from -0.09375 to 0.09375
- value_weight: bfloat16 [4096, 512], P('dp'), may hold values from -0.09375 to 0.09375
- query_gain: float32 [128], replicated, may hold values from 0.64 to 6.04
- key_gain: float32 [128], replicated, may hold values from 0.64 to 6.04
Outputs:
- grad_query: bfloat16 [8, 2048, 2048], P('dp', 'sp')
- grad_in: bfloat16 [8, 2048, 4096], P('dp', 'sp')
- grad_key_weight: float32 [4096, 512], P('dp')
- grad_value_weight: float32 [4096, 512], P('dp')
The draws below stay inside these ranges and needn't reach their ends.
All inputs are finite; a program needn't handle non-finite values.
Results may differ from the reference program's by a relative error of at most 0.018.
The reference program's roundings to bfloat16 on the way count: a program that leaves them out, or rounds other values in their place, can miss the bound.
Values may be sent and summed in bfloat16 or wider, within the bound.
A program may use at most 128 MiB of HBM per device.

```python
import math
from functools import partial
import jax
import jax.numpy as jnp
from jax import lax

D = 4096
HEADS = 16
KV_HEADS = 4
HEAD_DIM = 128
GRID_W = 64
TOK_DEV = 128
LEN = 2048
SEQS = 8
QW = 2048
KVW = 512
N_SP = 16
N_DP = 8


def gain_values(key, salt):
    base = jax.random.uniform(jax.random.fold_in(key, salt), (HEAD_DIM,), jnp.float32)
    return 0.64 + 0.72 * base


def draw_query_gain(key, part):
    return gain_values(key, 101)


def draw_key_gain(key, part):
    return gain_values(key, 102)


def drawn(key):
    seq_count = N_DP
    length = TOK_DEV * N_SP
    key_base = jnp.clip(jax.random.normal(jax.random.fold_in(key, 11), (seq_count, length, KV_HEADS * HEAD_DIM), jnp.float32), -6.0, 6.0)
    query_base = jnp.clip(jax.random.normal(jax.random.fold_in(key, 12), (seq_count, length, HEADS * HEAD_DIM), jnp.float32), -6.0, 6.0)
    return (jnp.clip(query_base, -9.0, 9.0), jnp.clip(key_base, -9.0, 9.0))


def draw_queries(key, part):
    return drawn(key)[0].astype(jnp.bfloat16)


def draw_keys(key, part):
    return drawn(key)[1].astype(jnp.bfloat16)


def spiked(entries, own_key, source, target, shards_of, factor):
    def block_of(dim):
        return (jnp.arange(entries.shape[dim]) // (entries.shape[dim] // shards_of)).reshape((-1,) + (1,) * (entries.ndim - 1 - dim))

    one_side = jax.random.permutation(own_key, shards_of)[block_of(target)]
    far = (block_of(target) + shards_of // 2) % shards_of
    return jnp.where((block_of(source) == one_side) | (block_of(source) == far), factor * entries, entries)


def level_of(own_key, extent, cuts, least, top_value):
    def one(dim, parts):
        heights = jax.random.uniform(jax.random.fold_in(jax.random.fold_in(own_key, 6), dim), (parts,), jnp.float32, least / len(cuts), top_value / len(cuts))
        return jnp.repeat(jnp.exp(heights), extent[dim] // parts).reshape((-1,) + (1,) * (len(extent) - dim - 1))

    loudness = one(*cuts[0])
    for cut in cuts[1:]:
        loudness = loudness * one(*cut)
    return loudness


def scatter_about(stream_key, dims, scale, reach, cuts=(), kind=jnp.bfloat16):
    values = jax.random.normal(stream_key, dims, jnp.float32) * scale
    if len(cuts) > 0:
        values = level_of(stream_key, dims, cuts, -0.22, 0.18) * values
    return jnp.clip(values, min=-reach, max=reach).astype(kind)


def heavy_noise(own_key, dims, width, most, cuts, heavy, kind=jnp.bfloat16):
    drawn = width * jax.random.normal(own_key, dims, jnp.float32)
    if cuts:
        drawn = drawn * level_of(own_key, dims, cuts, -0.22, 0.18)
    return jnp.clip(spiked(drawn, jax.random.fold_in(own_key, 3), *heavy), -most, most).astype(kind)


def setup_inputs(seed: int = 0) -> dict:
    key_of = jax.random.split(jax.random.key(seed), 10)
    return {
        "queries": draw_queries(jax.random.fold_in(key_of[9], 71), 0),
        "keys": draw_keys(jax.random.fold_in(key_of[9], 71), 0),
        "values": scatter_about(key_of[2], (SEQS, LEN, KVW), 1.0, 6.0, ((0, 8), (1, 16))),
        "out_grad": scatter_about(key_of[3], (SEQS, LEN, QW), 4.0, 24.0, ((0, 8), (1, 16))),
        "layer_in": heavy_noise(key_of[4], (SEQS, LEN, D), (2.0 / (N_DP * N_SP * TOK_DEV) ** 0.5), 0.09375, ((0, 8), (1, 16)), (1, 2, 16, 2.0)),
        "key_weight": scatter_about(key_of[5], (D, KVW), D ** -0.5, 0.09375, ((0, 8),)),
        "value_weight": scatter_about(key_of[6], (D, KVW), D ** -0.5, 0.09375, ((0, 8),)),
        "query_gain": draw_query_gain(jax.random.fold_in(key_of[9], 71), 0),
        "key_gain": draw_key_gain(jax.random.fold_in(key_of[9], 71), 0),
    }


epsilon = 1e-06
rope_base = 10000.0

def norm_rotate(vector, gain_vec, row_index, col_index):
    scaled = vector * lax.rsqrt(lax.optimization_barrier(jnp.mean(vector * vector, axis=-1, keepdims=True)) + epsilon) * gain_vec
    quarter = vector.shape[-1] // 4
    inverse = rope_base ** (-jnp.arange(quarter, dtype=jnp.float32) / quarter)
    pieces = []
    for offset, position in ((0, row_index), (2 * quarter, col_index)):
        angles = position.astype(jnp.float32)[:, None] * inverse[None, :]
        cosine = jnp.cos(angles)
        sine_part = jnp.sin(angles)
        first_half = scaled[:, offset:offset + quarter]
        second_half = scaled[:, offset + quarter:offset + 2 * quarter]
        pieces.append(first_half * cosine - second_half * sine_part)
        pieces.append(first_half * sine_part + second_half * cosine)
    return jnp.concatenate(pieces, axis=1)

def contract_cols(left_side, right_side):
    return lax.dot_general(left_side, right_side, (((1,), (1,)), ((), ())), preferred_element_type=jnp.float32)

def contract_rows(left_side, right_side):
    return lax.dot_general(left_side, right_side, (((0,), (0,)), ((), ())), preferred_element_type=jnp.float32)

def head_grads(query_rows, grad_rows, key_rows, value_rows, query_gain, key_gain):
    length = query_rows.shape[0]
    block_rows = math.gcd(length, 512)
    positions = jnp.arange(length, dtype=jnp.int32)
    row_index = positions // GRID_W
    col_index = positions % GRID_W
    q_rot, q_back = jax.vjp(partial(norm_rotate, gain_vec=query_gain, row_index=row_index, col_index=col_index), query_rows.astype(jnp.float32))
    k_rot, k_back = jax.vjp(partial(norm_rotate, gain_vec=key_gain, row_index=row_index, col_index=col_index), key_rows.astype(jnp.float32))
    q_bf = q_rot.astype(jnp.bfloat16)
    k_bf = k_rot.astype(jnp.bfloat16)
    score_scale = q_rot.shape[-1] ** (-0.5)

    def one_block(accums, block_index):
        k_acc, v_acc = accums
        row_start = block_index * block_rows
        q_block = lax.dynamic_slice_in_dim(q_bf, row_start, block_rows, 0)
        g_block = lax.dynamic_slice_in_dim(grad_rows, row_start, block_rows, 0)
        scores = contract_cols(q_block, k_bf) * score_scale
        shifted = jnp.exp(scores - lax.optimization_barrier(jnp.max(scores, axis=1, keepdims=True)))
        attn_probs = shifted / lax.optimization_barrier(jnp.sum(shifted, axis=1, keepdims=True))
        probs_b = attn_probs.astype(jnp.bfloat16)
        attn_out = jnp.dot(probs_b, value_rows, preferred_element_type=jnp.float32)
        row_delta = lax.optimization_barrier(jnp.sum(g_block.astype(jnp.float32) * attn_out, axis=1, keepdims=True))
        grad_probs = contract_cols(g_block, value_rows)
        grad_scores = (attn_probs * (grad_probs - row_delta)).astype(jnp.bfloat16)
        q_grad = jnp.dot(grad_scores, k_bf, preferred_element_type=jnp.float32) * score_scale
        k_acc = k_acc + contract_rows(grad_scores, q_block) * score_scale
        v_acc = v_acc + contract_rows(probs_b, g_block)
        return ((k_acc, v_acc), q_grad)
    zeros_init = jnp.zeros(query_rows.shape, jnp.float32)
    (k_acc, v_acc), q_grads = lax.scan(one_block, (zeros_init, zeros_init), jnp.arange(length // block_rows, dtype=jnp.int32))
    grad_rq = q_grads.reshape(length, query_rows.shape[1])
    grad_q = q_back(grad_rq)[0].astype(jnp.bfloat16)
    grad_k = k_back(k_acc)[0].astype(jnp.bfloat16)
    return (grad_q, grad_k, v_acc.astype(jnp.bfloat16))

def reference(queries, keys, values, out_grad, layer_in, key_weight, value_weight, query_gain, key_gain):
    seq_count, length, _ = queries.shape
    group_size = HEADS // KV_HEADS

    def by_head(array):
        return array.reshape(seq_count, length, HEADS, HEAD_DIM).transpose(0, 2, 1, 3).reshape(seq_count * HEADS, length, HEAD_DIM)

    def widened(array):
        spread = jnp.broadcast_to(array.reshape(seq_count, length, KV_HEADS, 1, HEAD_DIM), (seq_count, length, KV_HEADS, group_size, HEAD_DIM))
        return by_head(spread.reshape(seq_count, length, HEADS * HEAD_DIM))

    def one_head(items):
        return head_grads(items[0], items[1], items[2], items[3], query_gain, key_gain)
    grad_q, grad_k, grad_v = lax.map(one_head, (by_head(queries), by_head(out_grad), widened(keys), widened(values)))
    grad_query = grad_q.reshape(seq_count, HEADS, length, HEAD_DIM).transpose(0, 2, 1, 3).reshape(seq_count, length, HEADS * HEAD_DIM)

    def grouped(array):
        summed = lax.optimization_barrier(jnp.sum(array.reshape(seq_count, KV_HEADS, group_size, length, HEAD_DIM).astype(jnp.float32), axis=2))
        return summed.astype(jnp.bfloat16).transpose(0, 2, 1, 3).reshape(seq_count * length, KV_HEADS * HEAD_DIM)
    kv_grad = jnp.concatenate([grouped(grad_k), grouped(grad_v)], axis=1)
    both_weights = jnp.concatenate([key_weight, value_weight], axis=1)
    grad_in = contract_cols(kv_grad, both_weights).astype(jnp.bfloat16).reshape(seq_count, length, layer_in.shape[2])
    weight_grad = contract_rows(layer_in.reshape(seq_count * length, layer_in.shape[2]), kv_grad)
    kv_width = KV_HEADS * HEAD_DIM
    return (grad_query, grad_in, weight_grad[:, :kv_width], weight_grad[:, kv_width:])
```

```python
import functools

import jax
import jax.numpy as jnp
import numpy as np
from jax import lax
from jax.experimental import pallas as pl
from jax.experimental.pallas import tpu as pltpu
from jax.sharding import PartitionSpec as P

D = 128
GRID_W = 64
EPS = 1e-6
BASE = 10000.0
NZ = 4
NX = 4
NY = 4
NSP = NZ * NX
NDP = 2 * NY
T = 128
KC = 64
BF = jnp.bfloat16
F32 = jnp.float32
SCALE = D ** -0.5
EXP2_SCALE = float(SCALE * np.log2(np.e))


def rope_tables():
    quarter = D // 4
    inverse = np.float32(BASE) ** (-np.arange(quarter, dtype=np.float32) / np.float32(quarter))

    def one(count, half):
        angles = np.arange(count, dtype=np.float32)[:, None] * inverse[None, :]
        cosine, sine = np.cos(angles), np.sin(angles)
        table = np.zeros((3, count, D), np.float32)
        lo = half * 2 * quarter
        table[0, :, lo : lo + quarter] = cosine
        table[0, :, lo + quarter : lo + 2 * quarter] = cosine
        table[1, :, lo + quarter : lo + 2 * quarter] = sine
        table[2, :, lo : lo + quarter] = -sine
        return table

    rows = one(2048 // GRID_W, 0).reshape(3, 2048 // GRID_W, 1, D)
    cols = one(GRID_W, 1)
    return rows, cols


def rotate(n, c, s1, s2):
    return n * c + pltpu.roll(n, 32, 1) * s1 + pltpu.roll(n, 96, 1) * s2


def unrotate(n, c, s1, s2):
    return n * c - pltpu.roll(n, 32, 1) * s1 - pltpu.roll(n, 96, 1) * s2


def inv_rms(u):
    return lax.rsqrt(jnp.mean(u * u, axis=1, keepdims=True) + EPS)


def norm_back(grad, u, gain, c, s1, s2):
    r = inv_rms(u)
    t = unrotate(grad, c, s1, s2) * gain
    dot = jnp.sum(t * u, axis=1, keepdims=True)
    return r * t - u * (r * r * r * (1.0 / D) * dot)


def dot_nt(a, b):
    return lax.dot_general(a, b, (((1,), (1,)), ((), ())), preferred_element_type=F32)


def dot_nn(a, b):
    return lax.dot_general(a, b, (((1,), (0,)), ((), ())), preferred_element_type=F32)


def dot_tn(a, b):
    return lax.dot_general(a, b, (((0,), (0,)), ((), ())), preferred_element_type=F32)


def body(
    q, k, v, g, li, kw, vw, qg, kg, tr, tc,
    gq, gin, gw,
    q_all, g_all, k_all, v_all, k_src, k_t, tab, qs, gs, s_scr, dp_scr, pb, ds,
    dq_out, dv_src, dk_src, dv_in, dk_in, li_all, kw_s, vw_s, vs_all, ks_all,
    rs_src, rs_in, ag_src, gi_src,
    loc, zs, zr, xs, xr, lis, lir, dqs, dqr, dps, dpr, as_, ar, rss, rsr, ags, agr, gis, gir,
):
    sp = lax.axis_index("sp")
    dp = lax.axis_index("dp")
    z, x = sp // NX, lax.rem(sp, NX)
    y, core = dp // 2, lax.rem(dp, 2)

    def remote(src, dst, ss, rs, **where):
        return pltpu.make_async_remote_copy(
            src_ref=src, dst_ref=dst, send_sem=ss, recv_sem=rs,
            device_id=where, device_id_type=pl.DeviceIdType.MESH,
        )

    barrier = pltpu.get_barrier_semaphore()

    def greet_sp(o, _):
        pl.semaphore_signal(
            barrier, inc=1, device_id={"sp": lax.rem(sp + o, NSP)},
            device_id_type=pl.DeviceIdType.MESH,
        )
        return 0

    def greet_dp(o, _):
        pl.semaphore_signal(
            barrier, inc=1, device_id={"dp": lax.rem(dp + o, NDP)},
            device_id_type=pl.DeviceIdType.MESH,
        )
        return 0

    lax.fori_loop(1, NSP, greet_sp, 0)
    lax.fori_loop(1, NDP, greet_dp, 0)

    def cols(i, w):
        return pl.ds(pl.multiple_of(i * w, w), w)

    own = [
        pltpu.make_async_copy(q.at[:, cols(z, 512)], q_all.at[z], loc.at[0]),
        pltpu.make_async_copy(g.at[:, cols(z, 512)], g_all.at[z], loc.at[1]),
        pltpu.make_async_copy(v.at[:, cols(z, D)], v_all.at[x, z], loc.at[2]),
        pltpu.make_async_copy(li.at[:, cols(dp, 512)], li_all.at[dp], loc.at[3]),
        pltpu.make_async_copy(kw, kw_s, loc.at[4]),
        pltpu.make_async_copy(vw, vw_s, loc.at[5]),
    ]
    for c in own:
        c.start()

    for zz in range(NZ):
        shard = NX * zz + x
        for kind in range(3):
            part = tc[kind]
            tab[zz, kind, 0:64] = part + tr[kind, 2 * shard]
            tab[zz, kind, 64:128] = part + tr[kind, 2 * shard + 1]

    for h in range(NZ):
        u = k[:, h * D : (h + 1) * D].astype(F32)
        n = u * inv_rms(u) * kg[...]
        k_src[h] = rotate(n, tab[z, 0], tab[z, 1], tab[z, 2]).astype(BF)
    k_all[x, z] = k_src[z]

    pl.semaphore_wait(barrier, NSP + NDP - 2)

    def z_copies(o, side, kinds):
        peer = lax.rem(z + o, NZ)
        slot = z if side == "send" else peer
        pairs = (
            (k_src.at[peer], k_all.at[x, slot]),
            (v.at[:, cols(peer, D)], v_all.at[x, slot]),
            (q.at[:, cols(peer, 512)], q_all.at[slot]),
            (g.at[:, cols(peer, 512)], g_all.at[slot]),
        )
        return [
            remote(*pairs[i], zs.at[i, peer], zr.at[i, slot], sp=peer * NX + x) for i in kinds
        ]

    order = (1, 3, 2)
    for o in order:
        for c in z_copies(o, "send", (0, 1)):
            c.start()
    for o in order:
        for c in z_copies(o, "send", (2, 3)):
            c.start()

    def li_copy(o, side):
        peer = lax.rem(dp + o, NDP)
        slot = dp if side == "send" else peer
        return remote(li.at[:, cols(peer, 512)], li_all.at[slot], lis.at[peer], lir.at[slot], dp=peer)

    def li_start(o, _):
        li_copy(o, "send").start()
        return 0

    lax.fori_loop(1, NDP, li_start, 0)

    own[2].wait()
    for o in order:
        for c in z_copies(o, "recv", (0, 1)):
            c.wait_recv()

    def x_copies(o, side):
        peer = lax.rem(x + o, NX)
        slot = x if side == "send" else peer
        return [
            remote(k_all.at[slot], k_all.at[slot], xs.at[0, peer], xr.at[0, slot], sp=z * NX + peer),
            remote(v_all.at[slot], v_all.at[slot], xs.at[1, peer], xr.at[1, slot], sp=z * NX + peer),
        ]

    for o in order:
        for c in x_copies(o, "send"):
            c.start()
    own[0].wait()
    own[1].wait()
    for o in order:
        for c in x_copies(o, "recv"):
            c.wait_recv()
    k_t[...] = k_all[...].reshape(NSP * T, D).T

    def dq_copy(zz):
        return remote(dq_out.at[zz], gq.at[:, cols(z, 512)], dqs.at[zz], dqr.at[z], sp=zz * NX + x)

    def block(i, _):
        off = i // 2
        zz = lax.rem(z + off, NZ)
        pair = lax.rem(i, 2)

        @pl.when((pair == 0) & (off > 0))
        def _():
            remote(q.at[:, cols(z, 512)], q_all.at[zz], zs.at[2, zz], zr.at[2, zz], sp=zz * NX + x).wait_recv()
            remote(g.at[:, cols(z, 512)], g_all.at[zz], zs.at[3, zz], zr.at[3, zz], sp=zz * NX + x).wait_recv()

        c, s1, s2 = tab[zz, 0], tab[zz, 1], tab[zz, 2]
        wide = pl.ds(pl.multiple_of(pair * 256, 256), 256)
        rows = pl.ds(pl.multiple_of(i * 256, 256), 256)
        here = pl.ds(pl.multiple_of(i * 256, 256), 256)
        both = q_all[zz, :, wide].astype(F32)
        parts = []
        for h in range(2):
            u = both[:, h * D : (h + 1) * D]
            parts.append(rotate(u * inv_rms(u) * qg[...], c, s1, s2).astype(BF))
        qb = jnp.concatenate(parts, axis=0)
        qs[rows, :] = qb
        gb2 = g_all[zz, :, wide]
        gb = jnp.concatenate([gb2[:, :D], gb2[:, D:]], axis=0)
        gs[rows, :] = gb

        m8 = jnp.full((8, 256), -jnp.inf, F32)
        for j in range(8):
            kc = k_all[j // 2, 2 * (j % 2) : 2 * (j % 2) + 2].reshape(256, D)
            vc = v_all[j // 2, 2 * (j % 2) : 2 * (j % 2) + 2].reshape(256, D)
            s = dot_nt(kc, qb)
            s_scr[j * 256 : (j + 1) * 256, :] = s
            m8 = jnp.maximum(m8, jnp.max(s.reshape(32, 8, 256), axis=0))
            dp_scr[j * 256 : (j + 1) * 256, :] = dot_nt(vc, gb)
        m = jnp.max(m8, axis=0, keepdims=True)

        def exps(j, l8):
            at = pl.ds(pl.multiple_of(j * KC, KC), KC)
            e = jnp.exp2((s_scr[at, :] - m) * EXP2_SCALE)
            s_scr[at, :] = e
            return l8 + jnp.sum(e.reshape(KC // 8, 8, 256), axis=0)

        l8 = lax.fori_loop(0, 2048 // KC, exps, jnp.zeros((8, 256), F32), unroll=4)
        rl = 1.0 / jnp.sum(l8, axis=0, keepdims=True)

        def probs(j, d8):
            at = pl.ds(pl.multiple_of(j * KC, KC), KC)
            p = s_scr[at, :] * rl
            p_b = p.astype(BF)
            s_scr[at, :] = p
            pb[at, here] = p_b
            prod = p_b.astype(F32) * dp_scr[at, :]
            return d8 + jnp.sum(prod.reshape(KC // 8, 8, 256), axis=0)

        d8 = lax.fori_loop(0, 2048 // KC, probs, jnp.zeros((8, 256), F32), unroll=4)
        delta = jnp.sum(d8, axis=0, keepdims=True)

        def scores(j, _):
            at = pl.ds(pl.multiple_of(j * KC, KC), KC)
            ds[at, here] = (s_scr[at, :] * (dp_scr[at, :] - delta)).astype(BF)
            return 0

        lax.fori_loop(0, 2048 // KC, scores, 0, unroll=4)
        grad = dot_nn(k_t[...], ds[:, here]).T * SCALE
        outs = []
        for h in range(2):
            outs.append(
                norm_back(
                    grad[h * D : (h + 1) * D], both[:, h * D : (h + 1) * D], qg[...], c, s1, s2
                ).astype(BF)
            )
        dq_out[zz, :, wide] = jnp.concatenate(outs, axis=1)

        @pl.when(i == 1)
        def _():
            pltpu.make_async_copy(dq_out.at[z], gq.at[:, cols(z, 512)], loc.at[6]).start()

        @pl.when((pair == 1) & (off > 0))
        def _():
            dq_copy(zz).start()

        return 0

    lax.fori_loop(0, 8, block, 0)

    def grads_out(left, right, scale, src, into, which):
        def send(xx, zz):
            peer = zz * NX + xx
            return remote(
                src.at[xx, zz], into.at[sp], dps.at[which, peer], dpr.at[which, sp], sp=peer
            )

        def chunk(xx):
            at = pl.ds(pl.multiple_of(xx * 512, 512), 512)
            out = dot_nn(left[at, :], right[...])
            if scale is not None:
                out = out * scale
            src[xx] = out.astype(BF).reshape(NZ, T, D)

        def far(o, _):
            xx = lax.rem(x + o, NX)
            chunk(xx)
            for zz in range(NZ):
                send(xx, zz).start()
            return 0

        lax.fori_loop(1, NX, far, 0)
        chunk(x)
        for o in range(1, NZ):
            send(x, lax.rem(z + o, NZ)).start()
        into[sp] = src[x, z]

    grads_out(pb, gs, None, dv_src, dv_in, 0)
    grads_out(ds, qs, SCALE, dk_src, dk_in, 1)

    def wait_grads(src, into, which):
        def one(o, _):
            peer = lax.rem(sp + o, NSP)
            remote(src.at[0, 0], into.at[peer], dps.at[which, peer], dpr.at[which, peer], sp=peer).wait_recv()
            return 0

        lax.fori_loop(1, NSP, one, 0)

    def head_sum(into, h):
        total = into[NX * h].astype(F32)
        for xx in range(1, NX):
            total = total + into[NX * h + xx].astype(F32)
        return total

    def same(o, side, buf, which):
        peer = lax.rem(y + o, NY)
        slot = dp if side == "send" else 2 * peer + core
        return remote(buf.at[slot], buf.at[slot], as_.at[which, 2 * peer + core], ar.at[which, slot], dp=2 * peer + core)

    def cross(yy, side, buf, which):
        slot = 2 * yy + (core if side == "send" else 1 - core)
        return remote(buf.at[slot], buf.at[slot], as_.at[which + 2, yy], ar.at[which, slot], dp=2 * y + (1 - core))

    def gather_start(buf, which):
        for o in order:
            same(o, "send", buf, which).start()
        cross(y, "send", buf, which).start()

    def gather_finish(buf, which):
        for o in order:
            same(o, "recv", buf, which).wait_recv()
            cross(lax.rem(y + o, NY), "send", buf, which).start()
        for yy in range(NY):
            cross(yy, "recv", buf, which).wait_recv()

    wait_grads(dv_src, dv_in, 0)
    vs_all[dp] = jnp.concatenate([head_sum(dv_in, h).astype(BF) for h in range(NZ)], axis=1)
    gather_start(vs_all, 0)

    wait_grads(dk_src, dk_in, 1)
    pieces = []
    for h in range(NZ):
        u = k[:, h * D : (h + 1) * D].astype(F32)
        pieces.append(
            norm_back(head_sum(dk_in, h), u, kg[...], tab[z, 0], tab[z, 1], tab[z, 2]).astype(BF)
        )
    ks_all[dp] = jnp.concatenate(pieces, axis=1)
    gather_start(ks_all, 1)

    own[3].wait()

    def li_wait(o, _):
        li_copy(o, "recv").wait_recv()
        return 0

    lax.fori_loop(1, NDP, li_wait, 0)

    def reduce_start(buf, which):
        out = dot_tn(li_all[...].reshape(NDP * T, 512), buf[...].reshape(NDP * T, 512))
        rs_src[which] = out.astype(BF).reshape(NSP, 32, 512)
        rs_in[which, sp] = rs_src[which, sp]

        def one(o, _):
            peer = lax.rem(sp + o, NSP)
            remote(
                rs_src.at[which, peer], rs_in.at[which, sp], rss.at[which, peer], rsr.at[which, sp], sp=peer
            ).start()
            return 0

        lax.fori_loop(1, NSP, one, 0)

    def reduce_finish(which):
        def one(o, _):
            peer = lax.rem(sp + o, NSP)
            remote(
                rs_src.at[which, peer], rs_in.at[which, peer], rss.at[which, peer], rsr.at[which, peer], sp=peer
            ).wait_recv()
            return 0

        lax.fori_loop(1, NSP, one, 0)
        total = rs_in[which, 0].astype(F32)
        for i in range(1, NSP):
            total = total + rs_in[which, i].astype(F32)
        ag_src[which] = total.astype(BF)
        mine = pl.ds(pl.multiple_of(sp * 32, 32), 32)
        pltpu.make_async_copy(ag_src.at[which], gw.at[which, mine, :], loc.at[7 + which]).start()

        def two(o, _):
            peer = lax.rem(sp + o, NSP)
            remote(
                ag_src.at[which], gw.at[which, mine, :], ags.at[which, peer], agr.at[which, sp], sp=peer
            ).start()
            return 0

        lax.fori_loop(1, NSP, two, 0)

    gather_finish(vs_all, 0)
    reduce_start(vs_all, 0)
    gather_finish(ks_all, 1)
    reduce_start(ks_all, 1)

    own[4].wait()
    own[5].wait()

    def gi_copy(peer):
        return remote(gi_src.at[peer], gin.at[:, cols(dp, 512)], gis.at[peer], gir.at[dp], dp=peer)

    def grad_in(o, _):
        peer = lax.rem(dp + o, NDP)
        out = dot_nt(ks_all[peer], kw_s[...]) + dot_nt(vs_all[peer], vw_s[...])
        gi_src[peer] = out.astype(BF)

        @pl.when(o < NDP)
        def _():
            gi_copy(peer).start()

        return 0

    lax.fori_loop(1, NDP + 1, grad_in, 0)
    pltpu.make_async_copy(gi_src.at[dp], gin.at[:, cols(dp, 512)], loc.at[9]).start()

    reduce_finish(0)
    reduce_finish(1)

    pltpu.make_async_copy(dq_out.at[z], gq.at[:, cols(z, 512)], loc.at[6]).wait()
    pltpu.make_async_copy(gi_src.at[dp], gin.at[:, cols(dp, 512)], loc.at[9]).wait()
    mine = pl.ds(pl.multiple_of(sp * 32, 32), 32)
    for which in range(2):
        pltpu.make_async_copy(ag_src.at[which], gw.at[which, mine, :], loc.at[7 + which]).wait()
    for o in range(1, NZ):
        for c in z_copies(o, "send", (0, 1, 2, 3)):
            c.wait_send()
        for c in x_copies(o, "send"):
            c.wait_send()
        zz = lax.rem(z + o, NZ)
        dq_copy(zz).wait_send()
        remote(dq_out.at[zz], gq.at[:, cols(zz, 512)], dqs.at[zz], dqr.at[zz], sp=zz * NX + x).wait_recv()
    for which, buf in ((0, vs_all), (1, ks_all)):
        for o in range(1, NY):
            same(o, "send", buf, which).wait_send()
        for yy in range(NY):
            cross(yy, "send", buf, which).wait_send()

    def drain_dp(o, _):
        peer = lax.rem(dp + o, NDP)
        li_copy(o, "send").wait_send()
        gi_copy(peer).wait_send()
        remote(gi_src.at[peer], gin.at[:, cols(peer, 512)], gis.at[peer], gir.at[peer], dp=peer).wait_recv()
        return 0

    lax.fori_loop(1, NDP, drain_dp, 0)

    def drain_sp(o, _):
        peer = lax.rem(sp + o, NSP)
        theirs = pl.ds(pl.multiple_of(peer * 32, 32), 32)
        for which, src in ((0, dv_src), (1, dk_src)):
            remote(src.at[0, 0], dv_in.at[peer], dps.at[which, peer], dpr.at[which, peer], sp=peer).wait_send()
            remote(
                rs_src.at[which, peer], rs_in.at[which, peer], rss.at[which, peer], rsr.at[which, peer], sp=peer
            ).wait_send()
            c = remote(
                ag_src.at[which], gw.at[which, theirs, :], ags.at[which, peer], agr.at[which, peer], sp=peer
            )
            c.wait_send()
            c.wait_recv()
        return 0

    lax.fori_loop(1, NSP, drain_sp, 0)


def on_device(queries, keys, values, out_grad, layer_in, key_weight, value_weight, query_gain, key_gain):
    rows, cols = rope_tables()
    hbm = pl.BlockSpec(memory_space=pl.ANY)
    vmem = pl.BlockSpec(memory_space=pltpu.VMEM)
    dma = pltpu.SemaphoreType.DMA
    V = pltpu.VMEM
    gq, gin, gw = pl.pallas_call(
        body,
        out_shape=(
            jax.ShapeDtypeStruct((T, 2048), BF),
            jax.ShapeDtypeStruct((T, 4096), BF),
            jax.ShapeDtypeStruct((2, 512, 512), BF),
        ),
        in_specs=[hbm, vmem, hbm, hbm, hbm, hbm, hbm, vmem, vmem, vmem, vmem],
        out_specs=(hbm, hbm, hbm),
        scratch_shapes=[
            V((NZ, T, 512), BF),
            V((NZ, T, 512), BF),
            V((NX, NZ, T, D), BF),
            V((NX, NZ, T, D), BF),
            V((NZ, T, D), BF),
            V((D, 2048), BF),
            V((NZ, 3, T, D), F32),
            V((2048, D), BF),
            V((2048, D), BF),
            V((2048, 256), F32),
            V((2048, 256), F32),
            V((2048, 2048), BF),
            V((2048, 2048), BF),
            V((NZ, T, 512), BF),
            V((NX, NZ, T, D), BF),
            V((NX, NZ, T, D), BF),
            V((NSP, T, D), BF),
            V((NSP, T, D), BF),
            V((NDP, T, 512), BF),
            V((512, 512), BF),
            V((512, 512), BF),
            V((NDP, T, 512), BF),
            V((NDP, T, 512), BF),
            V((2, NSP, 32, 512), BF),
            V((2, NSP, 32, 512), BF),
            V((2, 32, 512), BF),
            V((NDP, T, 512), BF),
            dma((10,)),
            dma((4, NZ)),
            dma((4, NZ)),
            dma((2, NX)),
            dma((2, NX)),
            dma((NDP,)),
            dma((NDP,)),
            dma((NZ,)),
            dma((NZ,)),
            dma((2, NSP)),
            dma((2, NSP)),
            dma((4, NDP)),
            dma((2, NDP)),
            dma((2, NSP)),
            dma((2, NSP)),
            dma((2, NSP)),
            dma((2, NSP)),
            dma((NDP,)),
            dma((NDP,)),
        ],
        compiler_params=pltpu.CompilerParams(
            collective_id=0, has_side_effects=True, vmem_limit_bytes=60 * 1024 * 1024
        ),
        name="step",
    )(
        queries[0], keys[0], values[0], out_grad[0], layer_in[0], key_weight, value_weight,
        query_gain.reshape(1, D), key_gain.reshape(1, D), jnp.asarray(rows), jnp.asarray(cols),
    )
    return gq[None], gin[None], gw[1].astype(F32), gw[0].astype(F32)


def solution(mesh):
    in_specs = (
        P("dp", "sp", None),
        P("dp", "sp", None),
        P("dp", "sp", None),
        P("dp", "sp", None),
        P("dp", "sp", None),
        P("dp", None),
        P("dp", None),
        P(),
        P(),
    )
    out_specs = (P("dp", "sp", None), P("dp", "sp", None), P("dp", None), P("dp", None))
    return jax.shard_map(
        on_device, mesh=mesh, in_specs=in_specs, out_specs=out_specs, check_vma=False
    )
```

```python
import functools

import jax
import jax.numpy as jnp
import numpy as np
from jax import lax
from jax.experimental import pallas as pl
from jax.experimental.pallas import tpu as pltpu
from jax.sharding import PartitionSpec as P

D = 128
GRID_W = 64
EPS = 1e-6
BASE = 10000.0
NZ = 4
NX = 4
NY = 4
NSP = NZ * NX
NDP = 2 * NY
T = 128
KC = 64
BF = jnp.bfloat16
F32 = jnp.float32
SCALE = D ** -0.5
EXP2_SCALE = float(SCALE * np.log2(np.e))


def rope_tables():
    quarter = D // 4
    inverse = np.float32(BASE) ** (-np.arange(quarter, dtype=np.float32) / np.float32(quarter))

    def one(count, half):
        angles = np.arange(count, dtype=np.float32)[:, None] * inverse[None, :]
        cosine, sine = np.cos(angles), np.sin(angles)
        table = np.zeros((3, count, D), np.float32)
        lo = half * 2 * quarter
        table[0, :, lo : lo + quarter] = cosine
        table[0, :, lo + quarter : lo + 2 * quarter] = cosine
        table[1, :, lo + quarter : lo + 2 * quarter] = sine
        table[2, :, lo : lo + quarter] = -sine
        return table

    rows = one(2048 // GRID_W, 0).reshape(3, 2048 // GRID_W, 1, D)
    cols = one(GRID_W, 1)
    return rows, cols


def rotate(n, c, s1, s2):
    return n * c + pltpu.roll(n, 32, 1) * s1 + pltpu.roll(n, 96, 1) * s2


def unrotate(n, c, s1, s2):
    return n * c - pltpu.roll(n, 32, 1) * s1 - pltpu.roll(n, 96, 1) * s2


def inv_rms(u):
    return lax.rsqrt(jnp.mean(u * u, axis=1, keepdims=True) + EPS)


def norm_back(grad, u, gain, c, s1, s2):
    r = inv_rms(u)
    t = unrotate(grad, c, s1, s2) * gain
    dot = jnp.sum(t * u, axis=1, keepdims=True)
    return r * t - u * (r * r * r * (1.0 / D) * dot)


def dot_nt(a, b):
    return lax.dot_general(a, b, (((1,), (1,)), ((), ())), preferred_element_type=F32)


def dot_nn(a, b):
    return lax.dot_general(a, b, (((1,), (0,)), ((), ())), preferred_element_type=F32)


def dot_tn(a, b):
    return lax.dot_general(a, b, (((0,), (0,)), ((), ())), preferred_element_type=F32)


def body(
    q, k, v, g, li, kw, vw, qg, kg, tr, tc,
    gq, gin, gw,
    q_all, g_all, k_all, v_all, k_src, k_t, tab, qs, gs, m_scr, s_all, dp_all, pb,
    dq_out, dv_src, dk_src, dv_in, dk_in, li_all, kw_s, vw_s, vs_all, ks_all,
    rs_src, rs_in, ag_src, gi_src,
    loc, zs, zr, xs, xr, lis, lir, dqs, dqr, dps, dpr, as_, ar, rss, rsr, ags, agr, gis, gir,
):
    sp = lax.axis_index("sp")
    dp = lax.axis_index("dp")
    z, x = sp // NX, lax.rem(sp, NX)
    y, core = dp // 2, lax.rem(dp, 2)

    def remote(src, dst, ss, rs, **where):
        return pltpu.make_async_remote_copy(
            src_ref=src, dst_ref=dst, send_sem=ss, recv_sem=rs,
            device_id=where, device_id_type=pl.DeviceIdType.MESH,
        )

    barrier = pltpu.get_barrier_semaphore()

    def greet_sp(o, _):
        pl.semaphore_signal(
            barrier, inc=1, device_id={"sp": lax.rem(sp + o, NSP)},
            device_id_type=pl.DeviceIdType.MESH,
        )
        return 0

    def greet_dp(o, _):
        pl.semaphore_signal(
            barrier, inc=1, device_id={"dp": lax.rem(dp + o, NDP)},
            device_id_type=pl.DeviceIdType.MESH,
        )
        return 0

    lax.fori_loop(1, NSP, greet_sp, 0)
    lax.fori_loop(1, NDP, greet_dp, 0)

    def cols(i, w):
        return pl.ds(pl.multiple_of(i * w, w), w)

    own = [
        pltpu.make_async_copy(q.at[:, cols(z, 512)], q_all.at[z], loc.at[0]),
        pltpu.make_async_copy(g.at[:, cols(z, 512)], g_all.at[z], loc.at[1]),
        pltpu.make_async_copy(v.at[:, cols(z, D)], v_all.at[x, z], loc.at[2]),
        pltpu.make_async_copy(li.at[:, cols(dp, 512)], li_all.at[dp], loc.at[3]),
        pltpu.make_async_copy(kw, kw_s, loc.at[4]),
        pltpu.make_async_copy(vw, vw_s, loc.at[5]),
    ]
    for c in own:
        c.start()

    for zz in range(NZ):
        shard = NX * zz + x
        for kind in range(3):
            part = tc[kind]
            tab[zz, kind, 0:64] = part + tr[kind, 2 * shard]
            tab[zz, kind, 64:128] = part + tr[kind, 2 * shard + 1]

    for h in range(NZ):
        u = k[:, h * D : (h + 1) * D].astype(F32)
        n = u * inv_rms(u) * kg[...]
        k_src[h] = rotate(n, tab[z, 0], tab[z, 1], tab[z, 2]).astype(BF)
    k_all[x, z] = k_src[z]

    with jax.named_scope("s_barrier"):
        pl.semaphore_wait(barrier, NSP + NDP - 2)

    def z_copies(o, side, kinds):
        peer = lax.rem(z + o, NZ)
        slot = z if side == "send" else peer
        pairs = (
            (k_src.at[peer], k_all.at[x, slot]),
            (v.at[:, cols(peer, D)], v_all.at[x, slot]),
            (q.at[:, cols(peer, 512)], q_all.at[slot]),
            (g.at[:, cols(peer, 512)], g_all.at[slot]),
        )
        return [
            remote(*pairs[i], zs.at[i, peer], zr.at[i, slot], sp=peer * NX + x) for i in kinds
        ]

    order = (1, 3, 2)
    for o in order:
        for c in z_copies(o, "send", (0, 1)):
            c.start()
    for o in order:
        for c in z_copies(o, "send", (2, 3)):
            c.start()

    def li_copy(o, side):
        peer = lax.rem(dp + o, NDP)
        slot = dp if side == "send" else peer
        return remote(li.at[:, cols(peer, 512)], li_all.at[slot], lis.at[peer], lir.at[slot], dp=peer)

    def li_start(o, _):
        li_copy(o, "send").start()
        return 0

    lax.fori_loop(1, NDP, li_start, 0)

    own[2].wait()
    with jax.named_scope("s_zkv"):
        for o in order:
            for c in z_copies(o, "recv", (0, 1)):
                c.wait_recv()

    def x_copies(o, side):
        peer = lax.rem(x + o, NX)
        slot = x if side == "send" else peer
        return [
            remote(k_all.at[slot], k_all.at[slot], xs.at[0, peer], xr.at[0, slot], sp=z * NX + peer),
            remote(v_all.at[slot], v_all.at[slot], xs.at[1, peer], xr.at[1, slot], sp=z * NX + peer),
        ]

    for o in order:
        for c in x_copies(o, "send"):
            c.start()

    def dq_copy(zz):
        return remote(dq_out.at[zz], gq.at[:, cols(z, 512)], dqs.at[zz], dqr.at[z], sp=zz * NX + x)

    def prepare(o):
        zz = lax.rem(z + o, NZ)
        for h in range(4):
            rows = pl.ds(pl.multiple_of(o * 512 + h * T, T), T)
            u = q_all[zz, :, h * D : (h + 1) * D].astype(F32)
            n = u * inv_rms(u) * qg[...]
            qs[rows, :] = rotate(n, tab[zz, 0], tab[zz, 1], tab[zz, 2]).astype(BF)
            gs[rows, :] = g_all[zz, :, h * D : (h + 1) * D]

    def unit(xo, o):
        xx = lax.rem(x + xo, NX)
        qcols = pl.ds(pl.multiple_of(o * 512, 512), 512)
        qb, gb = qs[qcols, :], gs[qcols, :]
        for half in range(2):
            kc = k_all[xx, 2 * half : 2 * half + 2].reshape(256, D)
            vc = v_all[xx, 2 * half : 2 * half + 2].reshape(256, D)
            rows = pl.ds(pl.multiple_of(xx * 512 + half * 256, 256), 256)
            s = dot_nt(kc, qb)
            s_all[rows, qcols] = s
            m_scr[:, qcols] = jnp.maximum(m_scr[:, qcols], jnp.max(s.reshape(32, 8, 512), axis=0))
            dp_all[rows, qcols] = dot_nt(vc, gb)

    def wait_x(o):
        for c in x_copies(o, "recv"):
            c.wait_recv()

    def wait_q(o):
        for c in z_copies(o, "recv", (2, 3)):
            c.wait_recv()

    def three(i):
        return i + i // 2

    m_scr[...] = jnp.full((8, 2048), -jnp.inf, F32)
    own[0].wait()
    own[1].wait()
    with jax.named_scope("s_u0"):
        prepare(0)
        unit(0, 0)

    def near_keys(i, _):
        o = 1 + 2 * i
        wait_x(o)
        unit(o, 0)
        return 0

    with jax.named_scope("s_u1"):
        lax.fori_loop(0, 2, near_keys, 0)

    def near_queries(i, _):
        o = 1 + 2 * i
        wait_q(o)
        prepare(o)
        lax.fori_loop(0, 3, lambda j, _: (unit(three(j), o), 0)[1], 0)
        return 0

    with jax.named_scope("s_u2"):
        lax.fori_loop(0, 2, near_queries, 0)
    with jax.named_scope("s_u3"):
        wait_x(2)
        lax.fori_loop(0, 3, lambda j, _: (unit(2, three(j)), 0)[1], 0)
    with jax.named_scope("s_u4"):
        wait_q(2)
        prepare(2)
        lax.fori_loop(0, 4, lambda j, _: (unit(j, 2), 0)[1], 0)
        k_t[...] = k_all[...].reshape(NSP * T, D).T

    def soft(i, _):
        here = pl.ds(pl.multiple_of(i * 256, 256), 256)
        m = jnp.max(m_scr[:, here], axis=0, keepdims=True) * EXP2_SCALE

        def exps(j, l8):
            at = pl.ds(pl.multiple_of(j * KC, KC), KC)
            e = jnp.exp2(s_all[at, here] * EXP2_SCALE - m)
            s_all[at, here] = e
            return l8 + jnp.sum(e.reshape(KC // 8, 8, 256), axis=0)

        l8 = lax.fori_loop(0, 2048 // KC, exps, jnp.zeros((8, 256), F32), unroll=4)
        rl = 1.0 / jnp.sum(l8, axis=0, keepdims=True)

        def probs(j, _):
            at = pl.ds(pl.multiple_of(j * KC, KC), KC)
            p = s_all[at, here] * rl
            s_all[at, here] = p
            pb[at, here] = p.astype(BF)
            return 0

        lax.fori_loop(0, 2048 // KC, probs, 0, unroll=4)
        return 0

    with jax.named_scope("s_soft"):
        lax.fori_loop(0, 8, soft, 0)

    def grads_out(left, right, scale, src, into, which):
        def send(xx, zz):
            peer = zz * NX + xx
            return remote(
                src.at[xx, zz], into.at[sp], dps.at[which, peer], dpr.at[which, sp], sp=peer
            )

        def chunk(xx):
            at = pl.ds(pl.multiple_of(xx * 512, 512), 512)
            out = dot_nn(left[at, :], right[...])
            if scale is not None:
                out = out * scale
            src[xx] = out.astype(BF).reshape(NZ, T, D)

        def far(o, _):
            xx = lax.rem(x + o, NX)
            chunk(xx)
            for zz in range(NZ):
                send(xx, zz).start()
            return 0

        lax.fori_loop(1, NX, far, 0)
        chunk(x)
        for o in range(1, NZ):
            send(x, lax.rem(z + o, NZ)).start()
        into[sp] = src[x, z]

    def wait_grads(src, into, which):
        def one(o, _):
            peer = lax.rem(sp + o, NSP)
            remote(src.at[0, 0], into.at[peer], dps.at[which, peer], dpr.at[which, peer], sp=peer).wait_recv()
            return 0

        lax.fori_loop(1, NSP, one, 0)

    def head_sum(into, h):
        total = into[NX * h].astype(F32)
        for xx in range(1, NX):
            total = total + into[NX * h + xx].astype(F32)
        return total

    def same(o, side, buf, which):
        peer = lax.rem(y + o, NY)
        slot = dp if side == "send" else 2 * peer + core
        return remote(buf.at[slot], buf.at[slot], as_.at[which, 2 * peer + core], ar.at[which, slot], dp=2 * peer + core)

    def cross(yy, side, buf, which):
        slot = 2 * yy + (core if side == "send" else 1 - core)
        return remote(buf.at[slot], buf.at[slot], as_.at[which + 2, yy], ar.at[which, slot], dp=2 * y + (1 - core))

    def gather_start(buf, which):
        for o in order:
            same(o, "send", buf, which).start()
        cross(y, "send", buf, which).start()

    def gather_finish(buf, which):
        for o in order:
            same(o, "recv", buf, which).wait_recv()
            cross(lax.rem(y + o, NY), "send", buf, which).start()
        for yy in range(NY):
            cross(yy, "recv", buf, which).wait_recv()

    def reduce_start(buf, which):
        out = dot_tn(li_all[...].reshape(NDP * T, 512), buf[...].reshape(NDP * T, 512))
        rs_src[which] = out.astype(BF).reshape(NSP, 32, 512)
        rs_in[which, sp] = rs_src[which, sp]

        def one(o, _):
            peer = lax.rem(sp + o, NSP)
            remote(
                rs_src.at[which, peer], rs_in.at[which, sp], rss.at[which, peer], rsr.at[which, sp], sp=peer
            ).start()
            return 0

        lax.fori_loop(1, NSP, one, 0)

    def reduce_finish(which):
        def one(o, _):
            peer = lax.rem(sp + o, NSP)
            remote(
                rs_src.at[which, peer], rs_in.at[which, peer], rss.at[which, peer], rsr.at[which, peer], sp=peer
            ).wait_recv()
            return 0

        lax.fori_loop(1, NSP, one, 0)
        total = rs_in[which, 0].astype(F32)
        for i in range(1, NSP):
            total = total + rs_in[which, i].astype(F32)
        ag_src[which] = total.astype(BF)
        mine = pl.ds(pl.multiple_of(sp * 32, 32), 32)
        pltpu.make_async_copy(ag_src.at[which], gw.at[which, mine, :], loc.at[7 + which]).start()

        def two(o, _):
            peer = lax.rem(sp + o, NSP)
            remote(
                ag_src.at[which], gw.at[which, mine, :], ags.at[which, peer], agr.at[which, sp], sp=peer
            ).start()
            return 0

        lax.fori_loop(1, NSP, two, 0)

    with jax.named_scope("s_dv"):
        grads_out(pb, gs, None, dv_src, dv_in, 0)

    def back(i, _):
        off = i // 2
        zz = lax.rem(z + off, NZ)
        pair = lax.rem(i, 2)
        here = pl.ds(pl.multiple_of(i * 256, 256), 256)
        wide = pl.ds(pl.multiple_of(pair * 256, 256), 256)

        def deltas(j, d8):
            at = pl.ds(pl.multiple_of(j * KC, KC), KC)
            prod = pb[at, here].astype(F32) * dp_all[at, here]
            return d8 + jnp.sum(prod.reshape(KC // 8, 8, 256), axis=0)

        d8 = lax.fori_loop(0, 2048 // KC, deltas, jnp.zeros((8, 256), F32), unroll=4)
        delta = jnp.sum(d8, axis=0, keepdims=True)

        def scores(j, _):
            at = pl.ds(pl.multiple_of(j * KC, KC), KC)
            pb[at, here] = (s_all[at, here] * (dp_all[at, here] - delta)).astype(BF)
            return 0

        lax.fori_loop(0, 2048 // KC, scores, 0, unroll=4)
        grad = dot_nn(k_t[...], pb[:, here]).T * SCALE
        both = q_all[zz, :, wide].astype(F32)
        outs = []
        for h in range(2):
            outs.append(
                norm_back(
                    grad[h * D : (h + 1) * D], both[:, h * D : (h + 1) * D], qg[...],
                    tab[zz, 0], tab[zz, 1], tab[zz, 2],
                ).astype(BF)
            )
        dq_out[zz, :, wide] = jnp.concatenate(outs, axis=1)

        @pl.when(i == 1)
        def _():
            pltpu.make_async_copy(dq_out.at[z], gq.at[:, cols(z, 512)], loc.at[6]).start()

        @pl.when((pair == 1) & (off > 0))
        def _():
            dq_copy(zz).start()

        return 0

    with jax.named_scope("s_back"):
        lax.fori_loop(0, 8, back, 0)

    with jax.named_scope("s_wdv"):
        wait_grads(dv_src, dv_in, 0)
    vs_all[dp] = jnp.concatenate([head_sum(dv_in, h).astype(BF) for h in range(NZ)], axis=1)
    gather_start(vs_all, 0)
    with jax.named_scope("s_dk"):
        grads_out(pb, qs, SCALE, dk_src, dk_in, 1)

    own[3].wait()

    def li_wait(o, _):
        li_copy(o, "recv").wait_recv()
        return 0

    lax.fori_loop(1, NDP, li_wait, 0)

    with jax.named_scope("s_gfv"):
        gather_finish(vs_all, 0)
    with jax.named_scope("s_rsv"):
        reduce_start(vs_all, 0)

    with jax.named_scope("s_wdk"):
        wait_grads(dk_src, dk_in, 1)
    pieces = []
    for h in range(NZ):
        u = k[:, h * D : (h + 1) * D].astype(F32)
        pieces.append(
            norm_back(head_sum(dk_in, h), u, kg[...], tab[z, 0], tab[z, 1], tab[z, 2]).astype(BF)
        )
    ks_all[dp] = jnp.concatenate(pieces, axis=1)
    gather_start(ks_all, 1)

    with jax.named_scope("s_rfv"):
        reduce_finish(0)
    with jax.named_scope("s_gfk"):
        gather_finish(ks_all, 1)
    with jax.named_scope("s_rsk"):
        reduce_start(ks_all, 1)

    own[4].wait()
    own[5].wait()

    def gi_copy(peer):
        return remote(gi_src.at[peer], gin.at[:, cols(dp, 512)], gis.at[peer], gir.at[dp], dp=peer)

    def grad_in(o, _):
        peer = lax.rem(dp + o, NDP)
        out = dot_nt(ks_all[peer], kw_s[...]) + dot_nt(vs_all[peer], vw_s[...])
        gi_src[peer] = out.astype(BF)

        @pl.when(o < NDP)
        def _():
            gi_copy(peer).start()

        return 0

    with jax.named_scope("s_gin"):
        lax.fori_loop(1, NDP + 1, grad_in, 0)
    pltpu.make_async_copy(gi_src.at[dp], gin.at[:, cols(dp, 512)], loc.at[9]).start()

    with jax.named_scope("s_rfk"):
        reduce_finish(1)

    pltpu.make_async_copy(dq_out.at[z], gq.at[:, cols(z, 512)], loc.at[6]).wait()
    pltpu.make_async_copy(gi_src.at[dp], gin.at[:, cols(dp, 512)], loc.at[9]).wait()
    mine = pl.ds(pl.multiple_of(sp * 32, 32), 32)
    for which in range(2):
        pltpu.make_async_copy(ag_src.at[which], gw.at[which, mine, :], loc.at[7 + which]).wait()
    for o in range(1, NZ):
        for c in z_copies(o, "send", (0, 1, 2, 3)):
            c.wait_send()
        for c in x_copies(o, "send"):
            c.wait_send()
        zz = lax.rem(z + o, NZ)
        dq_copy(zz).wait_send()
        remote(dq_out.at[zz], gq.at[:, cols(zz, 512)], dqs.at[zz], dqr.at[zz], sp=zz * NX + x).wait_recv()
    for which, buf in ((0, vs_all), (1, ks_all)):
        for o in range(1, NY):
            same(o, "send", buf, which).wait_send()
        for yy in range(NY):
            cross(yy, "send", buf, which).wait_send()

    def drain_dp(o, _):
        peer = lax.rem(dp + o, NDP)
        li_copy(o, "send").wait_send()
        gi_copy(peer).wait_send()
        remote(gi_src.at[peer], gin.at[:, cols(peer, 512)], gis.at[peer], gir.at[peer], dp=peer).wait_recv()
        return 0

    with jax.named_scope("s_drdp"):
        lax.fori_loop(1, NDP, drain_dp, 0)

    def drain_sp(o, _):
        peer = lax.rem(sp + o, NSP)
        theirs = pl.ds(pl.multiple_of(peer * 32, 32), 32)
        for which, src in ((0, dv_src), (1, dk_src)):
            remote(src.at[0, 0], dv_in.at[peer], dps.at[which, peer], dpr.at[which, peer], sp=peer).wait_send()
            remote(
                rs_src.at[which, peer], rs_in.at[which, peer], rss.at[which, peer], rsr.at[which, peer], sp=peer
            ).wait_send()
            c = remote(
                ag_src.at[which], gw.at[which, theirs, :], ags.at[which, peer], agr.at[which, peer], sp=peer
            )
            c.wait_send()
            c.wait_recv()
        return 0

    with jax.named_scope("s_drsp"):
        lax.fori_loop(1, NSP, drain_sp, 0)


def on_device(queries, keys, values, out_grad, layer_in, key_weight, value_weight, query_gain, key_gain):
    rows, cols = rope_tables()
    hbm = pl.BlockSpec(memory_space=pl.ANY)
    vmem = pl.BlockSpec(memory_space=pltpu.VMEM)
    dma = pltpu.SemaphoreType.DMA
    V = pltpu.VMEM
    gq, gin, gw = pl.pallas_call(
        body,
        out_shape=(
            jax.ShapeDtypeStruct((T, 2048), BF),
            jax.ShapeDtypeStruct((T, 4096), BF),
            jax.ShapeDtypeStruct((2, 512, 512), BF),
        ),
        in_specs=[hbm, vmem, hbm, hbm, hbm, hbm, hbm, vmem, vmem, vmem, vmem],
        out_specs=(hbm, hbm, hbm),
        scratch_shapes=[
            V((NZ, T, 512), BF),
            V((NZ, T, 512), BF),
            V((NX, NZ, T, D), BF),
            V((NX, NZ, T, D), BF),
            V((NZ, T, D), BF),
            V((D, 2048), BF),
            V((NZ, 3, T, D), F32),
            V((2048, D), BF),
            V((2048, D), BF),
            V((8, 2048), F32),
            V((2048, 2048), F32),
            V((2048, 2048), F32),
            V((2048, 2048), BF),
            V((NZ, T, 512), BF),
            V((NX, NZ, T, D), BF),
            V((NX, NZ, T, D), BF),
            V((NSP, T, D), BF),
            V((NSP, T, D), BF),
            V((NDP, T, 512), BF),
            V((512, 512), BF),
            V((512, 512), BF),
            V((NDP, T, 512), BF),
            V((NDP, T, 512), BF),
            V((2, NSP, 32, 512), BF),
            V((2, NSP, 32, 512), BF),
            V((2, 32, 512), BF),
            V((NDP, T, 512), BF),
            dma((10,)),
            dma((4, NZ)),
            dma((4, NZ)),
            dma((2, NX)),
            dma((2, NX)),
            dma((NDP,)),
            dma((NDP,)),
            dma((NZ,)),
            dma((NZ,)),
            dma((2, NSP)),
            dma((2, NSP)),
            dma((4, NDP)),
            dma((2, NDP)),
            dma((2, NSP)),
            dma((2, NSP)),
            dma((2, NSP)),
            dma((2, NSP)),
            dma((NDP,)),
            dma((NDP,)),
        ],
        compiler_params=pltpu.CompilerParams(
            collective_id=0, has_side_effects=True, vmem_limit_bytes=63 * 1024 * 1024
        ),
        name="step",
    )(
        queries[0], keys[0], values[0], out_grad[0], layer_in[0], key_weight, value_weight,
        query_gain.reshape(1, D), key_gain.reshape(1, D), jnp.asarray(rows), jnp.asarray(cols),
    )
    return gq[None], gin[None], gw[1].astype(F32), gw[0].astype(F32)


def solution(mesh):
    in_specs = (
        P("dp", "sp", None),
        P("dp", "sp", None),
        P("dp", "sp", None),
        P("dp", "sp", None),
        P("dp", "sp", None),
        P("dp", None),
        P("dp", None),
        P(),
        P(),
    )
    out_specs = (P("dp", "sp", None), P("dp", "sp", None), P("dp", None), P("dp", None))
    return jax.shard_map(
        on_device, mesh=mesh, in_specs=in_specs, out_specs=out_specs, check_vma=False
    )
```

```python
import functools

import jax
import jax.numpy as jnp
import numpy as np
from jax import lax
from jax.experimental import pallas as pl
from jax.experimental.pallas import tpu as pltpu
from jax.sharding import PartitionSpec as P

D = 128
GRID_W = 64
EPS = 1e-6
BASE = 10000.0
NZ = 4
NX = 4
NY = 4
NSP = NZ * NX
NDP = 2 * NY
T = 128
KC = 64
BF = jnp.bfloat16
F32 = jnp.float32
SCALE = D ** -0.5
EXP2_SCALE = float(SCALE * np.log2(np.e))


def rope_tables():
    quarter = D // 4
    inverse = np.float32(BASE) ** (-np.arange(quarter, dtype=np.float32) / np.float32(quarter))

    def one(count, half):
        angles = np.arange(count, dtype=np.float32)[:, None] * inverse[None, :]
        cosine, sine = np.cos(angles), np.sin(angles)
        table = np.zeros((3, count, D), np.float32)
        lo = half * 2 * quarter
        table[0, :, lo : lo + quarter] = cosine
        table[0, :, lo + quarter : lo + 2 * quarter] = cosine
        table[1, :, lo + quarter : lo + 2 * quarter] = sine
        table[2, :, lo : lo + quarter] = -sine
        return table

    rows = one(2048 // GRID_W, 0).reshape(3, 2048 // GRID_W, 1, D)
    cols = one(GRID_W, 1)
    return rows, cols


def rotate(n, c, s1, s2):
    return n * c + pltpu.roll(n, 32, 1) * s1 + pltpu.roll(n, 96, 1) * s2


def unrotate(n, c, s1, s2):
    return n * c - pltpu.roll(n, 32, 1) * s1 - pltpu.roll(n, 96, 1) * s2


def inv_rms(u):
    return lax.rsqrt(jnp.mean(u * u, axis=1, keepdims=True) + EPS)


def norm_back(grad, u, gain, c, s1, s2):
    r = inv_rms(u)
    t = unrotate(grad, c, s1, s2) * gain
    dot = jnp.sum(t * u, axis=1, keepdims=True)
    return r * t - u * (r * r * r * (1.0 / D) * dot)


def dot_nt(a, b):
    return lax.dot_general(a, b, (((1,), (1,)), ((), ())), preferred_element_type=F32)


def dot_nn(a, b):
    return lax.dot_general(a, b, (((1,), (0,)), ((), ())), preferred_element_type=F32)


def dot_tn(a, b):
    return lax.dot_general(a, b, (((0,), (0,)), ((), ())), preferred_element_type=F32)


def body(
    q, k, v, g, li, kw, vw, qg, kg, tr, tc,
    gq, gin, gwv, gwk,
    q_all, g_all, k_all, v_all, k_src, k_t, tab, qs, gs, m_scr, rl_scr, d_scr, s_all, dp_all, pb, ds,
    dq_out, dv_src, dk_src, dv_in, dk_in, li_all, kw_s, vw_s, vs_all, ks_all,
    r1, st1, r2, go,
    loc, zs, zr, xs, xr, lis, lir, dqs, dqr, dps, dpr, as_, ar, ts, tr_, gis, gir,
):
    sp = lax.axis_index("sp")
    dp = lax.axis_index("dp")
    z, x = sp // NX, lax.rem(sp, NX)
    y, core = dp // 2, lax.rem(dp, 2)

    def remote(src, dst, ss, rs, **where):
        return pltpu.make_async_remote_copy(
            src_ref=src, dst_ref=dst, send_sem=ss, recv_sem=rs,
            device_id=where, device_id_type=pl.DeviceIdType.MESH,
        )

    barrier = pltpu.get_barrier_semaphore()

    def greet_sp(o, _):
        pl.semaphore_signal(
            barrier, inc=1, device_id={"sp": lax.rem(sp + o, NSP)},
            device_id_type=pl.DeviceIdType.MESH,
        )
        return 0

    def greet_dp(o, _):
        pl.semaphore_signal(
            barrier, inc=1, device_id={"dp": lax.rem(dp + o, NDP)},
            device_id_type=pl.DeviceIdType.MESH,
        )
        return 0

    lax.fori_loop(1, NSP, greet_sp, 0)
    lax.fori_loop(1, NDP, greet_dp, 0)

    def cols(i, w):
        return pl.ds(pl.multiple_of(i * w, w), w)

    own = [
        pltpu.make_async_copy(q.at[:, cols(z, 512)], q_all.at[z], loc.at[0]),
        pltpu.make_async_copy(g.at[:, cols(z, 512)], g_all.at[z], loc.at[1]),
        pltpu.make_async_copy(v.at[:, cols(z, D)], v_all.at[x, z], loc.at[2]),
        pltpu.make_async_copy(li.at[:, cols(dp, 512)], li_all.at[dp], loc.at[3]),
        pltpu.make_async_copy(kw, kw_s, loc.at[4]),
        pltpu.make_async_copy(vw, vw_s, loc.at[5]),
    ]
    for c in own:
        c.start()

    for zz in range(NZ):
        shard = NX * zz + x
        for kind in range(3):
            part = tc[kind]
            tab[zz, kind, 0:64] = part + tr[kind, 2 * shard]
            tab[zz, kind, 64:128] = part + tr[kind, 2 * shard + 1]

    for h in range(NZ):
        u = k[:, h * D : (h + 1) * D].astype(F32)
        n = u * inv_rms(u) * kg[...]
        k_src[h] = rotate(n, tab[z, 0], tab[z, 1], tab[z, 2]).astype(BF)
    k_all[x, z] = k_src[z]

    with jax.named_scope("s_barrier"):
        pl.semaphore_wait(barrier, NSP + NDP - 2)

    def z_copies(o, side, kinds):
        peer = lax.rem(z + o, NZ)
        slot = z if side == "send" else peer
        pairs = (
            (k_src.at[peer], k_all.at[x, slot]),
            (v.at[:, cols(peer, D)], v_all.at[x, slot]),
            (q.at[:, cols(peer, 512)], q_all.at[slot]),
            (g.at[:, cols(peer, 512)], g_all.at[slot]),
        )
        return [
            remote(*pairs[i], zs.at[i, peer], zr.at[i, slot], sp=peer * NX + x) for i in kinds
        ]

    order = (1, 3, 2)
    own[2].wait()
    for o in order:
        for c in z_copies(o, "send", (0, 1)):
            c.start()

    kv = (k_all, v_all)

    def x_copy(kind, chunk, zz, peer):
        sem = rem4(peer - chunk)
        return remote(
            kv[kind].at[chunk, zz], kv[kind].at[chunk, zz], xs.at[kind, sem, zz],
            xr.at[kind, chunk, zz], sp=z * NX + peer,
        )

    def rem4(i):
        return lax.rem(i + 4, 4)

    def x_send(zz):
        for kind in range(2):
            x_copy(kind, x, zz, rem4(x + 1)).start()
            x_copy(kind, x, zz, rem4(x - 1)).start()

    x_send(z)
    for o in order:
        for c in z_copies(o, "send", (2, 3)):
            c.start()

    def li_copy(o, side):
        peer = lax.rem(dp + o, NDP)
        slot = dp if side == "send" else peer
        return remote(li.at[:, cols(peer, 512)], li_all.at[slot], lis.at[peer], lir.at[slot], dp=peer)

    def li_start(o, _):
        li_copy(o, "send").start()
        return 0

    lax.fori_loop(1, NDP, li_start, 0)

    def dq_copy(zz):
        return remote(dq_out.at[zz], gq.at[:, cols(z, 512)], dqs.at[zz], dqr.at[z], sp=zz * NX + x)

    def prepare(o):
        zz = lax.rem(z + o, NZ)
        for h in range(4):
            rows = pl.ds(pl.multiple_of(o * 512 + h * T, T), T)
            u = q_all[zz, :, h * D : (h + 1) * D].astype(F32)
            n = u * inv_rms(u) * qg[...]
            qs[rows, :] = rotate(n, tab[zz, 0], tab[zz, 1], tab[zz, 2]).astype(BF)
            gs[rows, :] = g_all[zz, :, h * D : (h + 1) * D]

    def unit(xo, o):
        xx = lax.rem(x + xo, NX)
        qcols = pl.ds(pl.multiple_of(o * 512, 512), 512)
        qb, gb = qs[qcols, :], gs[qcols, :]
        for half in range(2):
            kc = k_all[xx, 2 * half : 2 * half + 2].reshape(256, D)
            vc = v_all[xx, 2 * half : 2 * half + 2].reshape(256, D)
            rows = pl.ds(pl.multiple_of(xx * 512 + half * 256, 256), 256)
            s = dot_nt(kc, qb)
            s_all[rows, qcols] = s
            m_scr[:, qcols] = jnp.maximum(m_scr[:, qcols], jnp.max(s.reshape(32, 8, 512), axis=0))
            dp_all[rows, qcols] = dot_nt(vc, gb)

    def x_wait(kind, o, zz):
        chunk = rem4(x + o)
        x_copy(kind, chunk, zz, chunk).wait_recv()

    def wait_q(o):
        for c in z_copies(o, "recv", (2, 3)):
            c.wait_recv()

    def three(i):
        return i + i // 2

    m_scr[...] = jnp.full((8, 2048), -jnp.inf, F32)
    own[0].wait()
    own[1].wait()
    prepare(0)
    with jax.named_scope("s_zkv"):
        for o in order:
            for c in z_copies(o, "recv", (0, 1)):
                c.wait_recv()
            x_send(rem4(z + o))
    with jax.named_scope("s_u0"):
        unit(0, 0)
    with jax.named_scope("s_u1"):
        for o in (0, 1, 3, 2):
            zz = rem4(z + o)
            x_wait(0, 1, zz)
            x_copy(0, rem4(x + 1), zz, rem4(x - 1)).start()
            x_wait(1, 3, zz)
            x_copy(1, rem4(x - 1), zz, rem4(x + 1)).start()
            x_wait(0, 3, zz)
            x_wait(1, 1, zz)
        unit(1, 0)
        unit(3, 0)

    def near_queries(i, _):
        o = 1 + 2 * i
        wait_q(o)
        prepare(o)
        lax.fori_loop(0, 3, lambda j, _: (unit(three(j), o), 0)[1], 0)
        return 0

    with jax.named_scope("s_u2"):
        lax.fori_loop(0, 2, near_queries, 0)
    with jax.named_scope("s_u3"):
        for o in (0, 1, 3, 2):
            for kind in range(2):
                x_wait(kind, 2, rem4(z + o))
        lax.fori_loop(0, 3, lambda j, _: (unit(2, three(j)), 0)[1], 0)
    with jax.named_scope("s_u4"):
        wait_q(2)
        prepare(2)
        lax.fori_loop(0, 4, lambda j, _: (unit(j, 2), 0)[1], 0)
        k_t[...] = k_all[...].reshape(NSP * T, D).T

    def block_cols(i):
        return pl.ds(pl.multiple_of(i * 256, 256), 256)

    def soft(i, _):
        here = block_cols(i)
        m = jnp.max(m_scr[:, here], axis=0, keepdims=True) * EXP2_SCALE
        l8 = jnp.zeros((8, 256), F32)
        for j in range(2048 // KC):
            e = jnp.exp2(s_all[j * KC : (j + 1) * KC, here] * EXP2_SCALE - m)
            s_all[j * KC : (j + 1) * KC, here] = e
            l8 = l8 + jnp.sum(e.reshape(KC // 8, 8, 256), axis=0)
        rl = 1.0 / jnp.sum(l8, axis=0, keepdims=True)
        rl_scr[:, here] = jnp.broadcast_to(rl, (8, 256))
        d8 = jnp.zeros((8, 256), F32)
        for j in range(2048 // KC):
            at = slice(j * KC, (j + 1) * KC)
            p_b = (s_all[at, here] * rl).astype(BF)
            pb[at, here] = p_b
            prod = p_b.astype(F32) * dp_all[at, here]
            d8 = d8 + jnp.sum(prod.reshape(KC // 8, 8, 256), axis=0)
        d_scr[:, here] = d8
        return 0

    with jax.named_scope("s_soft"):
        lax.fori_loop(0, 8, soft, 0)

    def grads_out(left, right, src, into, which):
        def step(t, _):
            xx = lax.rem(x + 1 + t // 2, NX)
            half = lax.rem(t, 2)
            at = pl.ds(pl.multiple_of(xx * 512 + half * 256, 256), 256)
            out = dot_nn(left[at, :], right[...])
            src[xx, pl.ds(2 * half, 2)] = out.astype(BF).reshape(2, T, D)
            for j in range(2):
                zz = 2 * half + j
                peer = zz * NX + xx

                @pl.when(peer != sp)
                def _():
                    remote(
                        src.at[xx, zz], into.at[sp], dps.at[which, peer], dpr.at[which, sp], sp=peer
                    ).start()

            return 0

        lax.fori_loop(0, 2 * NX, step, 0)
        into[sp] = src[x, z]

    def wait_grads(src, into, which):
        def one(o, _):
            peer = lax.rem(sp + o, NSP)
            remote(src.at[0, 0], into.at[peer], dps.at[which, peer], dpr.at[which, peer], sp=peer).wait_recv()
            return 0

        lax.fori_loop(1, NSP, one, 0)

    def head_sum(into, h):
        total = into[NX * h].astype(F32)
        for xx in range(1, NX):
            total = total + into[NX * h + xx].astype(F32)
        return total

    def same(o, side, buf, which):
        peer = lax.rem(y + o, NY)
        slot = dp if side == "send" else 2 * peer + core
        return remote(buf.at[slot], buf.at[slot], as_.at[which, 2 * peer + core], ar.at[which, slot], dp=2 * peer + core)

    def cross(yy, side, buf, which):
        slot = 2 * yy + (core if side == "send" else 1 - core)
        return remote(buf.at[slot], buf.at[slot], as_.at[which + 2, yy], ar.at[which, slot], dp=2 * y + (1 - core))

    def gather_start(buf, which):
        for o in order:
            same(o, "send", buf, which).start()
        cross(y, "send", buf, which).start()

    def gather_finish(buf, which):
        for o in order:
            same(o, "recv", buf, which).wait_recv()
            cross(lax.rem(y + o, NY), "send", buf, which).start()
        for yy in range(NY):
            cross(yy, "recv", buf, which).wait_recv()

    def gi_src(peer):
        return pb.at[pl.ds(pl.multiple_of(peer * T, T), T), 512:1024]

    outs = (gwv, gwk)

    def stage_copy(stage, which, half, o, side):
        along_x = (half == 0) == (stage in (0, 3))
        me = x if along_x else z
        peer = rem4(me + o)
        slot = me if side == "send" else peer
        wide = slice(half * 256, (half + 1) * 256)

        def rows(i, n, base=0):
            return pl.ds(pl.multiple_of(base + i * n, n), n)

        if stage == 0:
            src, dst = pb.at[rows(peer, T, which * 512), wide], r1.at[which, half, slot]
        elif stage == 1:
            src, dst = st1.at[which, half, rows(peer, 32)], r2.at[which, half, slot]
        elif stage == 2:
            src = dst = go.at[which, half, rows(slot, 32)]
        else:
            src, dst = go.at[which, half], outs[which].at[rows(slot, T), wide]
        target = z * NX + peer if along_x else peer * NX + x
        return remote(
            src, dst, ts.at[stage, which, half, peer], tr_.at[stage, which, half, slot], sp=target
        )

    def stage_start(stage, which, half):
        for o in order:
            stage_copy(stage, which, half, o, "send").start()

    def stage_wait(stage, which, half):
        for o in order:
            stage_copy(stage, which, half, o, "recv").wait_recv()

    def own_part(which, half):
        group = x if half == 0 else z
        return pltpu.make_async_copy(
            go.at[which, half],
            outs[which].at[cols(group, T), half * 256 : (half + 1) * 256],
            loc.at[7 + 2 * which + half],
        )

    def reduce_start(buf, which):
        out = dot_tn(li_all[...].reshape(NDP * T, 512), buf[...].reshape(NDP * T, 512))
        pb[which * 512 : (which + 1) * 512, 0:512] = out.astype(BF)
        for half in range(2):
            stage_start(0, which, half)

    def reduce_first(which):
        for half in range(2):
            me = x if half == 0 else z
            stage_wait(0, which, half)
            at = pl.ds(pl.multiple_of(which * 512 + me * T, T), T)
            total = pb[at, half * 256 : (half + 1) * 256].astype(F32)
            for o in order:
                total = total + r1[which, half, rem4(me + o)].astype(F32)
            st1[which, half] = total.astype(BF)
            stage_start(1, which, half)

    def reduce_second(which):
        for half in range(2):
            me = z if half == 0 else x
            stage_wait(1, which, half)
            at = pl.ds(pl.multiple_of(me * 32, 32), 32)
            total = st1[which, half, at].astype(F32)
            for o in order:
                total = total + r2[which, half, rem4(me + o)].astype(F32)
            go[which, half, at] = total.astype(BF)
            stage_start(2, which, half)

    def spread(which):
        for half in range(2):
            stage_wait(2, which, half)
            stage_start(3, which, half)
            own_part(which, half).start()

    def scores(t, _):
        here = block_cols(t)
        delta = jnp.sum(d_scr[:, here], axis=0, keepdims=True)
        rl = rl_scr[0:1, here]
        for j in range(2048 // KC):
            at = slice(j * KC, (j + 1) * KC)
            ds[at, here] = ((s_all[at, here] * rl) * (dp_all[at, here] - delta)).astype(BF)
        return 0

    with jax.named_scope("s_scores"):
        lax.fori_loop(0, 8, scores, 0)
    with jax.named_scope("s_dk"):
        grads_out(ds, qs, dk_src, dk_in, 1)
    with jax.named_scope("s_dv"):
        grads_out(pb, gs, dv_src, dv_in, 0)

    def query_grads(i):
        off = i // 2
        zz = lax.rem(z + off, NZ)
        pair = lax.rem(i, 2)
        wide = pl.ds(pl.multiple_of(pair * 256, 256), 256)
        grad = dot_nn(k_t[...], ds[:, block_cols(i)]).T * SCALE
        both = q_all[zz, :, wide].astype(F32)
        outs = []
        for h in range(2):
            outs.append(
                norm_back(
                    grad[h * D : (h + 1) * D], both[:, h * D : (h + 1) * D], qg[...],
                    tab[zz, 0], tab[zz, 1], tab[zz, 2],
                ).astype(BF)
            )
        dq_out[zz, :, wide] = jnp.concatenate(outs, axis=1)

    def query_send(i):
        off = i // 2
        zz = lax.rem(z + off, NZ)
        pair = lax.rem(i, 2)

        @pl.when(i == 1)
        def _():
            pltpu.make_async_copy(dq_out.at[z], gq.at[:, cols(z, 512)], loc.at[6]).start()

        @pl.when((pair == 1) & (off > 0))
        def _():
            dq_copy(zz).start()

    def back(t, _):
        query_grads(t)
        query_send(t)
        return 0

    with jax.named_scope("s_dq1"):
        lax.fori_loop(0, 4, back, 0)
    with jax.named_scope("s_wdk"):
        wait_grads(dk_src, dk_in, 1)
    pieces = []
    for h in range(NZ):
        u = k[:, h * D : (h + 1) * D].astype(F32)
        pieces.append(
            norm_back(head_sum(dk_in, h) * SCALE, u, kg[...], tab[z, 0], tab[z, 1], tab[z, 2]).astype(BF)
        )
    ks_all[dp] = jnp.concatenate(pieces, axis=1)
    gather_start(ks_all, 1)

    with jax.named_scope("s_dq2"):
        lax.fori_loop(4, 8, back, 0)
    with jax.named_scope("s_wdv"):
        wait_grads(dv_src, dv_in, 0)
    vs_all[dp] = jnp.concatenate([head_sum(dv_in, h).astype(BF) for h in range(NZ)], axis=1)
    gather_start(vs_all, 0)
    own[3].wait()

    def li_wait(o, _):
        li_copy(o, "recv").wait_recv()
        return 0

    lax.fori_loop(1, NDP, li_wait, 0)

    with jax.named_scope("s_gfk"):
        gather_finish(ks_all, 1)
    with jax.named_scope("s_rsk"):
        reduce_start(ks_all, 1)
    with jax.named_scope("s_gfv"):
        gather_finish(vs_all, 0)
    with jax.named_scope("s_rsv"):
        reduce_start(vs_all, 0)

    own[4].wait()
    own[5].wait()

    def gi_copy(peer):
        return remote(gi_src(peer), gin.at[:, cols(dp, 512)], gis.at[peer], gir.at[dp], dp=peer)

    def grad_in(i, _):
        group = lax.rem(dp // 4 + 1 + i, 2)
        four = pl.ds(4 * group, 4)
        out = dot_nt(ks_all[four].reshape(512, 512), kw_s[...])
        out = out + dot_nt(vs_all[four].reshape(512, 512), vw_s[...])
        pb[pl.ds(pl.multiple_of(group * 512, 512), 512), 512:1024] = out.astype(BF)
        for j in range(4):
            peer = 4 * group + j

            @pl.when(peer != dp)
            def _():
                gi_copy(peer).start()

        return 0

    with jax.named_scope("s_gin"):
        lax.fori_loop(0, 2, grad_in, 0)
    pltpu.make_async_copy(gi_src(dp), gin.at[:, cols(dp, 512)], loc.at[11]).start()

    with jax.named_scope("s_rf1"):
        reduce_first(1)
        reduce_first(0)
    with jax.named_scope("s_rf2"):
        reduce_second(1)
        reduce_second(0)
    with jax.named_scope("s_rf3"):
        spread(1)
        spread(0)

    pltpu.make_async_copy(dq_out.at[z], gq.at[:, cols(z, 512)], loc.at[6]).wait()
    pltpu.make_async_copy(gi_src(dp), gin.at[:, cols(dp, 512)], loc.at[11]).wait()
    for o in range(1, NZ):
        for c in z_copies(o, "send", (0, 1, 2, 3)):
            c.wait_send()
        zz = lax.rem(z + o, NZ)
        dq_copy(zz).wait_send()
        remote(dq_out.at[zz], gq.at[:, cols(zz, 512)], dqs.at[zz], dqr.at[zz], sp=zz * NX + x).wait_recv()
    for which, buf in ((0, vs_all), (1, ks_all)):
        for o in range(1, NY):
            same(o, "send", buf, which).wait_send()
        for yy in range(NY):
            cross(yy, "send", buf, which).wait_send()

    for zz in range(NZ):
        for kind in range(2):
            x_copy(kind, x, zz, rem4(x + 1)).wait_send()
            x_copy(kind, x, zz, rem4(x - 1)).wait_send()
        x_copy(0, rem4(x + 1), zz, rem4(x - 1)).wait_send()
        x_copy(1, rem4(x - 1), zz, rem4(x + 1)).wait_send()

    def drain_dp(o, _):
        peer = lax.rem(dp + o, NDP)
        li_copy(o, "send").wait_send()
        gi_copy(peer).wait_send()
        remote(gi_src(peer), gin.at[:, cols(peer, 512)], gis.at[peer], gir.at[peer], dp=peer).wait_recv()
        return 0

    with jax.named_scope("s_drdp"):
        lax.fori_loop(1, NDP, drain_dp, 0)

    def drain_sp(o, _):
        peer = lax.rem(sp + o, NSP)
        for which, src, into in ((0, dv_src, dv_in), (1, dk_src, dk_in)):
            remote(src.at[0, 0], into.at[peer], dps.at[which, peer], dpr.at[which, peer], sp=peer).wait_send()
        return 0

    lax.fori_loop(1, NSP, drain_sp, 0)
    with jax.named_scope("s_drsp"):
        for which in range(2):
            for half in range(2):
                stage_wait(3, which, half)
                own_part(which, half).wait()
                for stage in range(4):
                    for o in order:
                        stage_copy(stage, which, half, o, "send").wait_send()


def on_device(queries, keys, values, out_grad, layer_in, key_weight, value_weight, query_gain, key_gain):
    rows, cols = rope_tables()
    hbm = pl.BlockSpec(memory_space=pl.ANY)
    vmem = pl.BlockSpec(memory_space=pltpu.VMEM)
    dma = pltpu.SemaphoreType.DMA
    V = pltpu.VMEM
    gq, gin, gwv, gwk = pl.pallas_call(
        body,
        out_shape=(
            jax.ShapeDtypeStruct((T, 2048), BF),
            jax.ShapeDtypeStruct((T, 4096), BF),
            jax.ShapeDtypeStruct((512, 512), BF),
            jax.ShapeDtypeStruct((512, 512), BF),
        ),
        in_specs=[hbm, vmem, hbm, hbm, hbm, hbm, hbm, vmem, vmem, vmem, vmem],
        out_specs=(hbm, hbm, hbm, hbm),
        scratch_shapes=[
            V((NZ, T, 512), BF),
            V((NZ, T, 512), BF),
            V((NX, NZ, T, D), BF),
            V((NX, NZ, T, D), BF),
            V((NZ, T, D), BF),
            V((D, 2048), BF),
            V((NZ, 3, T, D), F32),
            V((2048, D), BF),
            V((2048, D), BF),
            V((8, 2048), F32),
            V((8, 2048), F32),
            V((8, 2048), F32),
            V((2048, 2048), F32),
            V((2048, 2048), F32),
            V((2048, 2048), BF),
            V((2048, 2048), BF),
            V((NZ, T, 512), BF),
            V((NX, NZ, T, D), BF),
            V((NX, NZ, T, D), BF),
            V((NSP, T, D), BF),
            V((NSP, T, D), BF),
            V((NDP, T, 512), BF),
            V((512, 512), BF),
            V((512, 512), BF),
            V((NDP, T, 512), BF),
            V((NDP, T, 512), BF),
            V((2, 2, 4, T, 256), BF),
            V((2, 2, T, 256), BF),
            V((2, 2, 4, 32, 256), BF),
            V((2, 2, T, 256), BF),
            dma((12,)),
            dma((4, NZ)),
            dma((4, NZ)),
            dma((2, NX, NZ)),
            dma((2, NX, NZ)),
            dma((NDP,)),
            dma((NDP,)),
            dma((NZ,)),
            dma((NZ,)),
            dma((2, NSP)),
            dma((2, NSP)),
            dma((4, NDP)),
            dma((2, NDP)),
            dma((4, 2, 2, 4)),
            dma((4, 2, 2, 4)),
            dma((NDP,)),
            dma((NDP,)),
        ],
        compiler_params=pltpu.CompilerParams(
            collective_id=0, has_side_effects=True, vmem_limit_bytes=67043328
        ),
        name="step",
    )(
        queries[0], keys[0], values[0], out_grad[0], layer_in[0], key_weight, value_weight,
        query_gain.reshape(1, D), key_gain.reshape(1, D), jnp.asarray(rows), jnp.asarray(cols),
    )
    return gq[None], gin[None], gwk.astype(F32), gwv.astype(F32)


def solution(mesh):
    in_specs = (
        P("dp", "sp", None),
        P("dp", "sp", None),
        P("dp", "sp", None),
        P("dp", "sp", None),
        P("dp", "sp", None),
        P("dp", None),
        P("dp", None),
        P(),
        P(),
    )
    out_specs = (P("dp", "sp", None), P("dp", "sp", None), P("dp", None), P("dp", None))
    return jax.shard_map(
        on_device, mesh=mesh, in_specs=in_specs, out_specs=out_specs, check_vma=False
    )
```

```python
import functools

import jax
import jax.numpy as jnp
import numpy as np
from jax import lax
from jax.experimental import pallas as pl
from jax.experimental.pallas import tpu as pltpu
from jax.sharding import PartitionSpec as P

D = 128
GRID_W = 64
EPS = 1e-6
BASE = 10000.0
NZ = 4
NX = 4
NY = 4
NSP = NZ * NX
NDP = 2 * NY
T = 128
KC = 64
BF = jnp.bfloat16
F32 = jnp.float32
SCALE = D ** -0.5
EXP2_SCALE = float(SCALE * np.log2(np.e))


def rope_tables():
    quarter = D // 4
    inverse = np.float32(BASE) ** (-np.arange(quarter, dtype=np.float32) / np.float32(quarter))

    def one(count, half):
        angles = np.arange(count, dtype=np.float32)[:, None] * inverse[None, :]
        cosine, sine = np.cos(angles), np.sin(angles)
        table = np.zeros((3, count, D), np.float32)
        lo = half * 2 * quarter
        table[0, :, lo : lo + quarter] = cosine
        table[0, :, lo + quarter : lo + 2 * quarter] = cosine
        table[1, :, lo + quarter : lo + 2 * quarter] = sine
        table[2, :, lo : lo + quarter] = -sine
        return table

    rows = one(2048 // GRID_W, 0).reshape(3, 2048 // GRID_W, 1, D)
    cols = one(GRID_W, 1)
    return rows, cols


def rotate(n, c, s1, s2):
    return n * c + pltpu.roll(n, 32, 1) * s1 + pltpu.roll(n, 96, 1) * s2


def unrotate(n, c, s1, s2):
    return n * c - pltpu.roll(n, 32, 1) * s1 - pltpu.roll(n, 96, 1) * s2


def inv_rms(u):
    return lax.rsqrt(jnp.mean(u * u, axis=1, keepdims=True) + EPS)


def norm_back(grad, u, gain, c, s1, s2):
    r = inv_rms(u)
    t = unrotate(grad, c, s1, s2) * gain
    dot = jnp.sum(t * u, axis=1, keepdims=True)
    return r * t - u * (r * r * r * (1.0 / D) * dot)


def dot_nt(a, b):
    return lax.dot_general(a, b, (((1,), (1,)), ((), ())), preferred_element_type=F32)


def dot_nn(a, b):
    return lax.dot_general(a, b, (((1,), (0,)), ((), ())), preferred_element_type=F32)


def dot_tn(a, b):
    return lax.dot_general(a, b, (((0,), (0,)), ((), ())), preferred_element_type=F32)


def body(
    q, k_in, v, g, li, kw, vw, qg_in, kg_in, tr_in, tc_in,
    gq, gin, gwv, gwk,
    k, qg, kg, tr, tc, q_all, g_all, k_all, v_all, k_src, k_t, tab, qs, gs, m_scr, rl_scr, d_scr, s_all, dp_all, pb, ds,
    dq_out, dv_src, dk_src, dv_in, dk_in, li_all, kw_s, vw_s, vs_all, ks_all,
    r1, st1, r2, go,
    loc, zs, zr, xs, xr, misc, dps, dpr, as_, ar, ts, trs,
):
    sp = lax.axis_index("sp")
    dp = lax.axis_index("dp")
    z, x = sp // NX, lax.rem(sp, NX)
    y, core = dp // 2, lax.rem(dp, 2)

    def remote(src, dst, ss, rs, **where):
        return pltpu.make_async_remote_copy(
            src_ref=src, dst_ref=dst, send_sem=ss, recv_sem=rs,
            device_id=where, device_id_type=pl.DeviceIdType.MESH,
        )

    def sent(ref, sem):
        remote(ref, ref, sem, sem, sp=sp).wait_send()

    def landed(ref, sem):
        remote(ref, ref, sem, sem, sp=sp).wait_recv()

    barrier = pltpu.get_barrier_semaphore()

    def greet_sp(o, _):
        pl.semaphore_signal(
            barrier, inc=1, device_id={"sp": lax.rem(sp + o, NSP)},
            device_id_type=pl.DeviceIdType.MESH,
        )
        return 0

    def greet_dp(o, _):
        pl.semaphore_signal(
            barrier, inc=1, device_id={"dp": lax.rem(dp + o, NDP)},
            device_id_type=pl.DeviceIdType.MESH,
        )
        return 0

    lax.fori_loop(1, NSP, greet_sp, 0)
    lax.fori_loop(1, NDP, greet_dp, 0)

    def cols(i, w):
        return pl.ds(pl.multiple_of(i * w, w), w)

    small = [
        pltpu.make_async_copy(src, dst, loc.at[7 + i])
        for i, (src, dst) in enumerate(
            ((k_in, k), (qg_in, qg), (kg_in, kg), (tr_in, tr), (tc_in, tc))
        )
    ]
    for c in small:
        c.start()
    own = [
        pltpu.make_async_copy(q.at[:, cols(z, 512)], q_all.at[z], loc.at[0]),
        pltpu.make_async_copy(g.at[:, cols(z, 512)], g_all.at[z], loc.at[1]),
        pltpu.make_async_copy(v.at[:, cols(z, D)], v_all.at[x, z], loc.at[2]),
        pltpu.make_async_copy(li.at[:, cols(dp, 512)], li_all.at[dp], loc.at[3]),
        pltpu.make_async_copy(kw, kw_s, loc.at[4]),
        pltpu.make_async_copy(vw, vw_s, loc.at[5]),
    ]
    for c in own:
        c.start()
    for c in small:
        c.wait()

    for zz in range(NZ):
        shard = NX * zz + x
        for kind in range(3):
            part = tc[kind]
            tab[zz, kind, 0:64] = part + tr[kind, 2 * shard]
            tab[zz, kind, 64:128] = part + tr[kind, 2 * shard + 1]

    for h in range(NZ):
        u = k[:, h * D : (h + 1) * D].astype(F32)
        n = u * inv_rms(u) * kg[...]
        k_src[h] = rotate(n, tab[z, 0], tab[z, 1], tab[z, 2]).astype(BF)
    k_all[x, z] = k_src[z]

    with jax.named_scope("s_barrier"):
        pl.semaphore_wait(barrier, NSP + NDP - 2)

    def z_copies(o, side, kinds):
        peer = lax.rem(z + o, NZ)
        slot = z if side == "send" else peer
        pairs = (
            (k_src.at[peer], k_all.at[x, slot]),
            (v.at[:, cols(peer, D)], v_all.at[x, slot]),
            (q.at[:, cols(peer, 512)], q_all.at[slot]),
            (g.at[:, cols(peer, 512)], g_all.at[slot]),
        )
        return [
            remote(*pairs[i], zs.at[i], zr.at[i // 2, slot], sp=peer * NX + x) for i in kinds
        ]

    order = (1, 3, 2)
    own[2].wait()
    for o in order:
        for c in z_copies(o, "send", (0, 1)):
            c.start()

    kv = (k_all, v_all)

    def rem4(i):
        return lax.rem(i + 4, 4)

    def x_copy(kind, chunk, zz, peer, ss, rs):
        at = kv[kind].at[chunk, zz]
        return remote(at, at, xs.at[ss], xr.at[rs], sp=z * NX + peer)

    def x_send(zz):
        x_copy(0, x, zz, rem4(x - 1), 0, zz).start()
        x_copy(1, x, zz, rem4(x + 1), 0, 4 + zz).start()
        x_copy(0, x, zz, rem4(x + 1), 0, 8).start()
        x_copy(1, x, zz, rem4(x - 1), 0, 8).start()

    x_send(z)
    for o in (1, 3):
        for c in z_copies(o, "send", (2, 3)):
            c.start()

    def li_copy(o, side):
        peer = lax.rem(dp + o, NDP)
        slot = dp if side == "send" else peer
        return remote(li.at[:, cols(peer, 512)], li_all.at[slot], misc.at[0], misc.at[1], dp=peer)

    def li_start(o, _):
        li_copy(o, "send").start()
        return 0

    lax.fori_loop(1, NDP, li_start, 0)

    def dq_copy(zz):
        return remote(dq_out.at[zz], gq.at[:, cols(z, 512)], misc.at[2], misc.at[3], sp=zz * NX + x)

    def prepare(o):
        zz = lax.rem(z + o, NZ)
        for h in range(4):
            rows = pl.ds(pl.multiple_of(o * 512 + h * T, T), T)
            u = q_all[zz, :, h * D : (h + 1) * D].astype(F32)
            n = u * inv_rms(u) * qg[...]
            qs[rows, :] = rotate(n, tab[zz, 0], tab[zz, 1], tab[zz, 2]).astype(BF)
            gs[rows, :] = g_all[zz, :, h * D : (h + 1) * D]

    def unit(xo, o):
        xx = lax.rem(x + xo, NX)
        qcols = pl.ds(pl.multiple_of(o * 512, 512), 512)
        qb, gb = qs[qcols, :], gs[qcols, :]
        for half in range(2):
            kc = k_all[xx, 2 * half : 2 * half + 2].reshape(256, D)
            vc = v_all[xx, 2 * half : 2 * half + 2].reshape(256, D)
            rows = pl.ds(pl.multiple_of(xx * 512 + half * 256, 256), 256)
            s = dot_nt(kc, qb)
            s_all[rows, qcols] = s
            m_scr[:, qcols] = jnp.maximum(m_scr[:, qcols], jnp.max(s.reshape(32, 8, 512), axis=0))
            dp_all[rows, qcols] = dot_nt(vc, gb)

    m_scr[...] = jnp.full((8, 2048), -jnp.inf, F32)
    own[0].wait()
    own[1].wait()
    def block_cols(i):
        return pl.ds(pl.multiple_of(i * 256, 256), 256)

    def soft(i):
        here = block_cols(i)
        m = jnp.max(m_scr[:, here], axis=0, keepdims=True) * EXP2_SCALE
        l8 = jnp.zeros((8, 256), F32)
        for j in range(2048 // KC):
            e = jnp.exp2(s_all[j * KC : (j + 1) * KC, here] * EXP2_SCALE - m)
            s_all[j * KC : (j + 1) * KC, here] = e
            l8 = l8 + jnp.sum(e.reshape(KC // 8, 8, 256), axis=0)
        rl = 1.0 / jnp.sum(l8, axis=0, keepdims=True)
        rl_scr[:, here] = jnp.broadcast_to(rl, (8, 256))
        d8 = jnp.zeros((8, 256), F32)
        for j in range(2048 // KC):
            at = slice(j * KC, (j + 1) * KC)
            p_b = (s_all[at, here] * rl).astype(BF)
            pb[at, here] = p_b
            prod = p_b.astype(F32) * dp_all[at, here]
            d8 = d8 + jnp.sum(prod.reshape(KC // 8, 8, 256), axis=0)
        d_scr[:, here] = d8

    def scores(t):
        here = block_cols(t)
        delta = jnp.sum(d_scr[:, here], axis=0, keepdims=True)
        rl = rl_scr[0:1, here]
        for j in range(2048 // KC):
            at = slice(j * KC, (j + 1) * KC)
            ds[at, here] = ((s_all[at, here] * rl) * (dp_all[at, here] - delta)).astype(BF)

    prepare(0)
    with jax.named_scope("s_zkv"):
        for o in order:
            landed(k_src.at[0:2], zr.at[0, rem4(z + o)])
            x_send(rem4(z + o))
        for c in z_copies(2, "send", (2, 3)):
            c.start()
    with jax.named_scope("s_u0"):
        unit(0, 0)
    with jax.named_scope("s_u1"):
        for o in (0, 1, 3, 2):
            zz = rem4(z + o)
            landed(k_src.at[0], xr.at[zz])
            x_copy(0, rem4(x + 1), zz, rem4(x - 1), 1, 9).start()
            landed(k_src.at[0], xr.at[4 + zz])
            x_copy(1, rem4(x - 1), zz, rem4(x + 1), 1, 9).start()
        landed(k_all.at[0:2], xr.at[8])
        unit(1, 0)
        unit(3, 0)
        landed(k_all.at[0:2], xr.at[9])
        unit(2, 0)

    def block(i, _):
        soft(i)
        scores(i)
        return 0

    with jax.named_scope("s_b0"):
        lax.fori_loop(0, 2, block, 0)

    def shard(i, _):
        o = 1 + 2 * i - 3 * (i // 2)
        with jax.named_scope("s_qw"):
            landed(q_all.at[0:2], zr.at[1, rem4(z + o)])
        prepare(o)
        lax.fori_loop(0, 4, lambda j, _: (unit(j, o), 0)[1], 0)
        lax.fori_loop(2 * o, 2 * o + 2, block, 0)
        return 0

    with jax.named_scope("s_b1"):
        lax.fori_loop(0, 3, shard, 0)
    k_t[...] = k_all[...].reshape(NSP * T, D).T
    def grads_out(left, right, src, into, which):
        def step(t, _):
            xx = lax.rem(x + 1 + t // 2, NX)
            half = lax.rem(t, 2)
            at = pl.ds(pl.multiple_of(xx * 512 + half * 256, 256), 256)
            out = dot_nn(left[at, :], right[...])
            src[xx, pl.ds(2 * half, 2)] = out.astype(BF).reshape(2, T, D)
            for j in range(2):
                zz = 2 * half + j
                peer = zz * NX + xx

                @pl.when(peer != sp)
                def _():
                    remote(
                        src.at[xx, zz], into.at[sp], dps.at[which], dpr.at[which], sp=peer
                    ).start()

            return 0

        lax.fori_loop(0, 2 * NX, step, 0)
        into[sp] = src[x, z]

    def wait_grads(into, which):
        landed(into.at[0 : NSP - 1], dpr.at[which])

    def head_sum(into, h):
        total = into[NX * h].astype(F32)
        for xx in range(1, NX):
            total = total + into[NX * h + xx].astype(F32)
        return total

    def same(o, buf, which):
        peer = rem4(y + o)
        return remote(
            buf.at[dp], buf.at[dp], as_.at[which], ar.at[which, y], dp=2 * peer + core
        )

    def cross(yy, buf, which):
        slot = 2 * yy + core
        return remote(
            buf.at[slot], buf.at[slot], as_.at[which], ar.at[which, 4], dp=2 * y + (1 - core)
        )

    def gather_start(buf, which):
        for o in order:
            same(o, buf, which).start()
        cross(y, buf, which).start()

    def gather_finish(buf, which):
        for o in order:
            yy = rem4(y + o)
            landed(buf.at[0], ar.at[which, yy])
            cross(yy, buf, which).start()
        landed(buf.at[0:4], ar.at[which, 4])

    def gi_src(peer):
        return pb.at[pl.ds(pl.multiple_of(peer * T, T), T), 512:1024]

    outs = (gwv, gwk)

    def stage_copy(stage, which, half, o):
        along_x = (half == 0) == (stage != 1)
        me = x if along_x else z
        peer = rem4(me + o)
        wide = slice(half * 256, (half + 1) * 256)
        if stage == 0:
            src = pb.at[pl.ds(pl.multiple_of(which * 512 + peer * T, T), T), wide]
            dst = r1.at[which, half, me]
        elif stage == 1:
            src, dst = st1.at[which, half], r2.at[which, half, me]
        else:
            src, dst = go.at[which, half], outs[which].at[cols(me, T), wide]
        target = z * NX + peer if along_x else peer * NX + x
        return remote(src, dst, ts.at[stage], trs.at[stage, which, half], sp=target)

    def stage_start(stage, which, half):
        for o in order:
            stage_copy(stage, which, half, o).start()

    def stage_wait(stage, which, half):
        landed(r1.at[which, half, 0:3], trs.at[stage, which, half])

    def own_part(which, half):
        return pltpu.make_async_copy(
            go.at[which, half],
            outs[which].at[cols(x if half == 0 else z, T), half * 256 : (half + 1) * 256],
            loc.at[12 + 2 * which + half],
        )

    def reduce_start(buf, which):
        out = dot_tn(li_all[...].reshape(NDP * T, 512), buf[...].reshape(NDP * T, 512))
        pb[which * 512 : (which + 1) * 512, 0:512] = out.astype(BF)
        for half in range(2):
            stage_start(0, which, half)

    def reduce_first(which):
        for half in range(2):
            me = x if half == 0 else z
            stage_wait(0, which, half)
            at = pl.ds(pl.multiple_of(which * 512 + me * T, T), T)
            total = pb[at, half * 256 : (half + 1) * 256].astype(F32)
            for o in order:
                total = total + r1[which, half, rem4(me + o)].astype(F32)
            st1[which, half] = total.astype(BF)
            stage_start(1, which, half)

    def reduce_second(which):
        for half in range(2):
            me = z if half == 0 else x
            stage_wait(1, which, half)
            total = st1[which, half].astype(F32)
            for o in order:
                total = total + r2[which, half, rem4(me + o)].astype(F32)
            go[which, half] = total.astype(BF)
            stage_start(2, which, half)
            own_part(which, half).start()

    with jax.named_scope("s_dk"):
        grads_out(ds, qs, dk_src, dk_in, 1)
    with jax.named_scope("s_dv"):
        grads_out(pb, gs, dv_src, dv_in, 0)

    def query_grads(i):
        off = i // 2
        zz = lax.rem(z + off, NZ)
        pair = lax.rem(i, 2)
        wide = pl.ds(pl.multiple_of(pair * 256, 256), 256)
        grad = dot_nn(k_t[...], ds[:, block_cols(i)]).T * SCALE
        both = q_all[zz, :, wide].astype(F32)
        outs = []
        for h in range(2):
            outs.append(
                norm_back(
                    grad[h * D : (h + 1) * D], both[:, h * D : (h + 1) * D], qg[...],
                    tab[zz, 0], tab[zz, 1], tab[zz, 2],
                ).astype(BF)
            )
        dq_out[zz, :, wide] = jnp.concatenate(outs, axis=1)

    def query_send(i):
        off = i // 2
        zz = lax.rem(z + off, NZ)
        pair = lax.rem(i, 2)

        @pl.when(i == 1)
        def _():
            pltpu.make_async_copy(dq_out.at[z], gq.at[:, cols(z, 512)], loc.at[6]).start()

        @pl.when((pair == 1) & (off > 0))
        def _():
            dq_copy(zz).start()

    def back(t, _):
        query_grads(t)
        query_send(t)
        return 0

    with jax.named_scope("s_dq1"):
        lax.fori_loop(0, 4, back, 0)
    with jax.named_scope("s_wdk"):
        wait_grads(dk_in, 1)
    pieces = []
    for h in range(NZ):
        u = k[:, h * D : (h + 1) * D].astype(F32)
        pieces.append(
            norm_back(head_sum(dk_in, h) * SCALE, u, kg[...], tab[z, 0], tab[z, 1], tab[z, 2]).astype(BF)
        )
    ks_all[dp] = jnp.concatenate(pieces, axis=1)
    gather_start(ks_all, 1)

    with jax.named_scope("s_dq2"):
        lax.fori_loop(4, 8, back, 0)
    with jax.named_scope("s_wdv"):
        wait_grads(dv_in, 0)
    vs_all[dp] = jnp.concatenate([head_sum(dv_in, h).astype(BF) for h in range(NZ)], axis=1)
    gather_start(vs_all, 0)
    own[3].wait()

    landed(li_all.at[0 : NDP - 1], misc.at[1])
    with jax.named_scope("s_gfk"):
        gather_finish(ks_all, 1)
    with jax.named_scope("s_rsk"):
        reduce_start(ks_all, 1)
    with jax.named_scope("s_gfv"):
        gather_finish(vs_all, 0)
    with jax.named_scope("s_rsv"):
        reduce_start(vs_all, 0)

    own[4].wait()
    own[5].wait()

    def gi_copy(peer):
        return remote(gi_src(peer), gin.at[:, cols(dp, 512)], misc.at[4], misc.at[5], dp=peer)

    def grad_in(i, _):
        group = lax.rem(dp // 4 + 1 + i, 2)
        four = pl.ds(4 * group, 4)
        out = dot_nt(ks_all[four].reshape(512, 512), kw_s[...])
        out = out + dot_nt(vs_all[four].reshape(512, 512), vw_s[...])
        pb[pl.ds(pl.multiple_of(group * 512, 512), 512), 512:1024] = out.astype(BF)
        for j in range(4):
            peer = 4 * group + j

            @pl.when(peer != dp)
            def _():
                gi_copy(peer).start()

        return 0

    with jax.named_scope("s_gin"):
        lax.fori_loop(0, 2, grad_in, 0)
    pltpu.make_async_copy(gi_src(dp), gin.at[:, cols(dp, 512)], loc.at[16]).start()

    with jax.named_scope("s_rf1"):
        reduce_first(1)
        reduce_first(0)
    with jax.named_scope("s_rf2"):
        reduce_second(1)
        reduce_second(0)
    sent(k_src.at[0:3], zs.at[0])
    sent(k_src.at[0:3], zs.at[1])
    sent(q_all.at[0:3], zs.at[2])
    sent(q_all.at[0:3], zs.at[3])
    sent(k_all, xs.at[0])
    sent(k_all.at[0:2], xs.at[1])
    sent(li_all.at[0 : NDP - 1], misc.at[0])
    sent(dq_out.at[0:3], misc.at[2])
    landed(dq_out.at[0:3], misc.at[3])
    for which, buf in ((0, vs_all), (1, ks_all)):
        sent(dv_in.at[0 : NSP - 1], dps.at[which])
        sent(buf.at[0 : NDP - 1], as_.at[which])
    pltpu.make_async_copy(dq_out.at[z], gq.at[:, cols(z, 512)], loc.at[6]).wait()
    pltpu.make_async_copy(gi_src(dp), gin.at[:, cols(dp, 512)], loc.at[16]).wait()
    with jax.named_scope("s_drdp"):
        sent(li_all.at[0 : NDP - 1], misc.at[4])
        landed(li_all.at[0 : NDP - 1], misc.at[5])
    with jax.named_scope("s_drsp"):
        for which in (1, 0):
            for half in range(2):
                stage_wait(2, which, half)
                own_part(which, half).wait()
        for stage in range(3):
            sent(r1.at[:, :, 0:3], ts.at[stage])


def finish(gq_in, gin_in, gwv_in, gwk_in, gq, gin, gwv, gwk, a, b, c, e, sem):
    ins, outs = [], []
    for i in range(4):
        at = slice(i * 32, (i + 1) * 32)
        rows = slice(i * T, (i + 1) * T)
        ins.append(
            [
                pltpu.make_async_copy(gwk_in.at[rows], c.at[0, rows], sem.at[0, i, 0]),
                pltpu.make_async_copy(gwv_in.at[rows], c.at[1, rows], sem.at[0, i, 1]),
                pltpu.make_async_copy(gin_in.at[at], b.at[at], sem.at[0, i, 2]),
                pltpu.make_async_copy(gq_in.at[at], a.at[at], sem.at[0, i, 3]),
            ]
        )
        outs.append(
            [
                pltpu.make_async_copy(e.at[0, rows], gwk.at[rows], sem.at[1, i, 0]),
                pltpu.make_async_copy(e.at[1, rows], gwv.at[rows], sem.at[1, i, 1]),
                pltpu.make_async_copy(b.at[at], gin.at[at], sem.at[1, i, 2]),
                pltpu.make_async_copy(a.at[at], gq.at[at], sem.at[1, i, 3]),
            ]
        )
    for group in ins:
        for copy in group:
            copy.start()
    for i in range(4):
        rows = slice(i * T, (i + 1) * T)
        for j in range(4):
            ins[i][j].wait()
            if j < 2:
                e[j, rows] = c[j, rows].astype(F32)
            outs[i][j].start()
    for group in outs:
        for copy in group:
            copy.wait()


def on_device(queries, keys, values, out_grad, layer_in, key_weight, value_weight, query_gain, key_gain):
    rows, cols = rope_tables()
    hbm = pl.BlockSpec(memory_space=pl.ANY)
    dma = pltpu.SemaphoreType.DMA
    V = pltpu.VMEM
    gq, gin, gwv, gwk = pl.pallas_call(
        body,
        out_shape=(
            jax.ShapeDtypeStruct((T, 2048), BF),
            jax.ShapeDtypeStruct((T, 4096), BF),
            jax.ShapeDtypeStruct((512, 512), BF),
            jax.ShapeDtypeStruct((512, 512), BF),
        ),
        in_specs=[hbm] * 11,
        out_specs=(hbm, hbm, hbm, hbm),
        scratch_shapes=[
            V((T, 512), BF),
            V((1, D), F32),
            V((1, D), F32),
            V(rows.shape, F32),
            V(cols.shape, F32),
            V((NZ, T, 512), BF),
            V((NZ, T, 512), BF),
            V((NX, NZ, T, D), BF),
            V((NX, NZ, T, D), BF),
            V((NZ, T, D), BF),
            V((D, 2048), BF),
            V((NZ, 3, T, D), F32),
            V((2048, D), BF),
            V((2048, D), BF),
            V((8, 2048), F32),
            V((8, 2048), F32),
            V((8, 2048), F32),
            V((2048, 2048), F32),
            V((2048, 2048), F32),
            V((2048, 2048), BF),
            V((2048, 2048), BF),
            V((NZ, T, 512), BF),
            V((NX, NZ, T, D), BF),
            V((NX, NZ, T, D), BF),
            V((NSP, T, D), BF),
            V((NSP, T, D), BF),
            V((NDP, T, 512), BF),
            V((512, 512), BF),
            V((512, 512), BF),
            V((NDP, T, 512), BF),
            V((NDP, T, 512), BF),
            V((2, 2, 4, T, 256), BF),
            V((2, 2, T, 256), BF),
            V((2, 2, 4, T, 256), BF),
            V((2, 2, T, 256), BF),
            dma((17,)),
            dma((4,)),
            dma((2, NZ)),
            dma((2,)),
            dma((10,)),
            dma((6,)),
            dma((2,)),
            dma((2,)),
            dma((2,)),
            dma((2, 5)),
            dma((3,)),
            dma((3, 2, 2)),
        ],
        compiler_params=pltpu.CompilerParams(
            collective_id=0, has_side_effects=True, vmem_limit_bytes=67043328
        ),
        name="step",
    )(
        queries[0], keys[0], values[0], out_grad[0], layer_in[0], key_weight, value_weight,
        query_gain.reshape(1, D), key_gain.reshape(1, D), jnp.asarray(rows), jnp.asarray(cols),
    )
    gq, gin, gwv, gwk = pl.pallas_call(
        finish,
        out_shape=(
            jax.ShapeDtypeStruct((T, 2048), BF),
            jax.ShapeDtypeStruct((T, 4096), BF),
            jax.ShapeDtypeStruct((512, 512), F32),
            jax.ShapeDtypeStruct((512, 512), F32),
        ),
        in_specs=[hbm] * 4,
        out_specs=(hbm,) * 4,
        scratch_shapes=[
            V((T, 2048), BF),
            V((T, 4096), BF),
            V((2, 512, 512), BF),
            V((2, 512, 512), F32),
            dma((2, 4, 4)),
        ],
        name="finish",
    )(gq, gin, gwv, gwk)
    return gq[None], gin[None], gwk, gwv


def solution(mesh):
    in_specs = (
        P("dp", "sp", None),
        P("dp", "sp", None),
        P("dp", "sp", None),
        P("dp", "sp", None),
        P("dp", "sp", None),
        P("dp", None),
        P("dp", None),
        P(),
        P(),
    )
    out_specs = (P("dp", "sp", None), P("dp", "sp", None), P("dp", None), P("dp", None))
    return jax.shard_map(
        on_device, mesh=mesh, in_specs=in_specs, out_specs=out_specs, check_vma=False
    )
```

```python
import functools

import jax
import jax.numpy as jnp
import numpy as np
from jax import lax
from jax.experimental import pallas as pl
from jax.experimental.pallas import tpu as pltpu
from jax.sharding import PartitionSpec as P

D = 128
GRID_W = 64
EPS = 1e-6
BASE = 10000.0
NZ = 4
NX = 4
NY = 4
NSP = NZ * NX
NDP = 2 * NY
T = 128
KC = 64
BF = jnp.bfloat16
F32 = jnp.float32
SCALE = D ** -0.5
EXP2_SCALE = float(SCALE * np.log2(np.e))


def rope_tables():
    quarter = D // 4
    inverse = np.float32(BASE) ** (-np.arange(quarter, dtype=np.float32) / np.float32(quarter))

    def one(count, half):
        angles = np.arange(count, dtype=np.float32)[:, None] * inverse[None, :]
        cosine, sine = np.cos(angles), np.sin(angles)
        table = np.zeros((3, count, D), np.float32)
        lo = half * 2 * quarter
        table[0, :, lo : lo + quarter] = cosine
        table[0, :, lo + quarter : lo + 2 * quarter] = cosine
        table[1, :, lo + quarter : lo + 2 * quarter] = sine
        table[2, :, lo : lo + quarter] = -sine
        return table

    rows = one(2048 // GRID_W, 0).reshape(3, 2048 // GRID_W, 1, D)
    cols = one(GRID_W, 1)
    return rows, cols


def rotate(n, c, s1, s2):
    return n * c + pltpu.roll(n, 32, 1) * s1 + pltpu.roll(n, 96, 1) * s2


def unrotate(n, c, s1, s2):
    return n * c - pltpu.roll(n, 32, 1) * s1 - pltpu.roll(n, 96, 1) * s2


def inv_rms(u):
    return lax.rsqrt(jnp.mean(u * u, axis=1, keepdims=True) + EPS)


def norm_back(grad, u, gain, c, s1, s2):
    r = inv_rms(u)
    t = unrotate(grad, c, s1, s2) * gain
    dot = jnp.sum(t * u, axis=1, keepdims=True)
    return r * t - u * (r * r * r * (1.0 / D) * dot)


def dot_nt(a, b):
    return lax.dot_general(a, b, (((1,), (1,)), ((), ())), preferred_element_type=F32)


def dot_nn(a, b):
    return lax.dot_general(a, b, (((1,), (0,)), ((), ())), preferred_element_type=F32)


def dot_tn(a, b):
    return lax.dot_general(a, b, (((0,), (0,)), ((), ())), preferred_element_type=F32)


def body(
    q, k_in, v, g, li, kw, vw, qg_in, kg_in, tr_in, tc_in,
    gq, gin, gwv, gwk,
    k, qg, kg, tr, tc, q_all, g_all, k_all, v_all, k_src, k_t, tab, qs, gs, m_scr, rl_scr, d_scr, s_all, dp_all, pb, ds,
    dq_out, dk_src, dv_in, dk_in, li_all, kw_s, vw_s, vs_all, ks_all,
    r1, st1, r2, go,
    loc, zs, zr, xs, xr, misc, dps, dpr, as_, ar, ts, trs,
):
    sp = lax.axis_index("sp")
    dp = lax.axis_index("dp")
    z, x = sp // NX, lax.rem(sp, NX)
    y, core = dp // 2, lax.rem(dp, 2)

    def remote(src, dst, ss, rs, **where):
        return pltpu.make_async_remote_copy(
            src_ref=src, dst_ref=dst, send_sem=ss, recv_sem=rs,
            device_id=where, device_id_type=pl.DeviceIdType.MESH,
        )

    def sent(ref, sem):
        remote(ref, ref, sem, sem, sp=sp).wait_send()

    def landed(ref, sem):
        remote(ref, ref, sem, sem, sp=sp).wait_recv()

    barrier = pltpu.get_barrier_semaphore()

    def greet_sp(o, _):
        pl.semaphore_signal(
            barrier, inc=1, device_id={"sp": lax.rem(sp + o, NSP)},
            device_id_type=pl.DeviceIdType.MESH,
        )
        return 0

    def greet_dp(o, _):
        pl.semaphore_signal(
            barrier, inc=1, device_id={"dp": lax.rem(dp + o, NDP)},
            device_id_type=pl.DeviceIdType.MESH,
        )
        return 0

    lax.fori_loop(1, NSP, greet_sp, 0)
    lax.fori_loop(1, NDP, greet_dp, 0)

    def cols(i, w):
        return pl.ds(pl.multiple_of(i * w, w), w)

    small = [
        pltpu.make_async_copy(src, dst, loc.at[7 + i])
        for i, (src, dst) in enumerate(
            ((k_in, k), (qg_in, qg), (kg_in, kg), (tr_in, tr), (tc_in, tc))
        )
    ]
    for c in small:
        c.start()
    own = [
        pltpu.make_async_copy(q.at[:, cols(z, 512)], q_all.at[z], loc.at[0]),
        pltpu.make_async_copy(g.at[:, cols(z, 512)], g_all.at[z], loc.at[1]),
        pltpu.make_async_copy(v.at[:, cols(z, D)], v_all.at[x, z], loc.at[2]),
        pltpu.make_async_copy(li.at[:, cols(dp, 512)], li_all.at[dp], loc.at[3]),
        pltpu.make_async_copy(kw, kw_s, loc.at[4]),
        pltpu.make_async_copy(vw, vw_s, loc.at[5]),
    ]
    for c in own:
        c.start()
    for c in small:
        c.wait()

    for zz in range(NZ):
        shard = NX * zz + x
        for kind in range(3):
            part = tc[kind]
            tab[zz, kind, 0:64] = part + tr[kind, 2 * shard]
            tab[zz, kind, 64:128] = part + tr[kind, 2 * shard + 1]

    for h in range(NZ):
        u = k[:, h * D : (h + 1) * D].astype(F32)
        n = u * inv_rms(u) * kg[...]
        k_src[h] = rotate(n, tab[z, 0], tab[z, 1], tab[z, 2]).astype(BF)
    k_all[x, z] = k_src[z]

    with jax.named_scope("s_barrier"):
        pl.semaphore_wait(barrier, NSP + NDP - 2)

    def z_copies(o, side, kinds):
        peer = lax.rem(z + o, NZ)
        slot = z if side == "send" else peer
        pairs = (
            (k_src.at[peer], k_all.at[x, slot]),
            (v.at[:, cols(peer, D)], v_all.at[x, slot]),
            (q.at[:, cols(peer, 512)], q_all.at[slot]),
            (g.at[:, cols(peer, 512)], g_all.at[slot]),
        )
        return [
            remote(*pairs[i], zs.at[i], zr.at[i // 2, slot], sp=peer * NX + x) for i in kinds
        ]

    order = (1, 3, 2)
    own[2].wait()
    for o in order:
        for c in z_copies(o, "send", (0, 1)):
            c.start()

    kv = (k_all, v_all)

    def rem4(i):
        return lax.rem(i + 4, 4)

    def x_copy(kind, chunk, zz, peer, ss, rs):
        at = kv[kind].at[chunk, zz]
        return remote(at, at, xs.at[ss], xr.at[rs], sp=z * NX + peer)

    def x_send(zz):
        x_copy(0, x, zz, rem4(x - 1), 0, zz).start()
        x_copy(1, x, zz, rem4(x + 1), 0, 4 + zz).start()
        x_copy(0, x, zz, rem4(x + 1), 0, 8).start()
        x_copy(1, x, zz, rem4(x - 1), 0, 8).start()

    x_send(z)
    for o in (1, 3):
        for c in z_copies(o, "send", (2, 3)):
            c.start()

    def li_copy(o, side):
        peer = lax.rem(dp + o, NDP)
        slot = dp if side == "send" else peer
        return remote(li.at[:, cols(peer, 512)], li_all.at[slot], misc.at[0], misc.at[1], dp=peer)

    def li_start(o, _):
        li_copy(o, "send").start()
        return 0

    lax.fori_loop(1, NDP, li_start, 0)

    def dq_copy(zz):
        return remote(dq_out.at[zz], gq.at[:, cols(z, 512)], misc.at[2], misc.at[3], sp=zz * NX + x)

    def prepare(o):
        zz = lax.rem(z + o, NZ)
        for h in range(4):
            rows = pl.ds(pl.multiple_of(o * 512 + h * T, T), T)
            u = q_all[zz, :, h * D : (h + 1) * D].astype(F32)
            n = u * inv_rms(u) * qg[...]
            qs[rows, :] = rotate(n, tab[zz, 0], tab[zz, 1], tab[zz, 2]).astype(BF)
            gs[rows, :] = g_all[zz, :, h * D : (h + 1) * D]

    def unit(xo, o):
        xx = lax.rem(x + xo, NX)
        qcols = pl.ds(pl.multiple_of(o * 512, 512), 512)
        qb, gb = qs[qcols, :], gs[qcols, :]
        for half in range(2):
            kc = k_all[xx, 2 * half : 2 * half + 2].reshape(256, D)
            vc = v_all[xx, 2 * half : 2 * half + 2].reshape(256, D)
            rows = pl.ds(pl.multiple_of(xx * 512 + half * 256, 256), 256)
            s = dot_nt(kc, qb)
            s_all[2 * o, rows, :] = s[:, :256]
            s_all[2 * o + 1, rows, :] = s[:, 256:]
            m_scr[:, qcols] = jnp.maximum(m_scr[:, qcols], jnp.max(s.reshape(32, 8, 512), axis=0))
            w = dot_nt(vc, gb)
            dp_all[2 * o, rows, :] = w[:, :256]
            dp_all[2 * o + 1, rows, :] = w[:, 256:]

    m_scr[...] = jnp.full((8, 2048), -jnp.inf, F32)
    own[0].wait()
    own[1].wait()
    def block_cols(i):
        return pl.ds(pl.multiple_of(i * 256, 256), 256)

    def exps(i, j, m, l8):
        at = slice(j * KC, (j + 1) * KC)
        e = jnp.exp2(s_all[i, at, :] * EXP2_SCALE - m)
        s_all[i, at, :] = e
        return l8 + jnp.sum(e.reshape(KC // 8, 8, 256), axis=0)

    def soft(i):
        m = jnp.max(m_scr[:, block_cols(i)], axis=0, keepdims=True) * EXP2_SCALE
        l8 = jnp.zeros((8, 256), F32)
        for j in range(2048 // KC):
            l8 = exps(i, j, m, l8)
        probs(i, l8)

    def whole(i):
        rows = pl.ds(pl.multiple_of(i * 256, 256), 256)
        qb, gb = qs[rows, :], gs[rows, :]
        m8 = jnp.full((8, 256), -jnp.inf, F32)
        for j in range(NX):
            s = dot_nt(k_all[j].reshape(512, D), qb)
            s_all[i, j * 512 : (j + 1) * 512, :] = s
            m8 = jnp.maximum(m8, jnp.max(s.reshape(64, 8, 256), axis=0))
        m = jnp.max(m8, axis=0, keepdims=True) * EXP2_SCALE
        l8 = jnp.zeros((8, 256), F32)
        for j in range(2 * NX):
            vb = v_all[j // 2, 2 * (j % 2) : 2 * (j % 2) + 2].reshape(256, D)
            dp_all[i, j * 256 : (j + 1) * 256, :] = dot_nt(vb, gb)
            for n in range(4):
                l8 = exps(i, 4 * j + n, m, l8)
        probs(i, l8)

    def probs(i, l8):
        here = block_cols(i)
        rl = 1.0 / jnp.sum(l8, axis=0, keepdims=True)
        rl_scr[:, here] = jnp.broadcast_to(rl, (8, 256))
        d8 = jnp.zeros((8, 256), F32)
        for j in range(2048 // KC):
            at = slice(j * KC, (j + 1) * KC)
            p_b = (s_all[i, at, :] * rl).astype(BF)
            pb[i, at, :] = p_b
            prod = p_b.astype(F32) * dp_all[i, at, :]
            d8 = d8 + jnp.sum(prod.reshape(KC // 8, 8, 256), axis=0)
        d_scr[:, here] = d8

    def scores(i):
        here = block_cols(i)
        delta = jnp.sum(d_scr[:, here], axis=0, keepdims=True)
        rl = rl_scr[0:1, here]
        for j in range(2048 // KC):
            at = slice(j * KC, (j + 1) * KC)
            ds[i, at, :] = ((s_all[i, at, :] * rl) * (dp_all[i, at, :] - delta)).astype(BF)

    prepare(0)
    with jax.named_scope("s_zkv"):
        for o in order:
            landed(k_src.at[0:2], zr.at[0, rem4(z + o)])
            x_send(rem4(z + o))
        for c in z_copies(2, "send", (2, 3)):
            c.start()
    with jax.named_scope("s_u0"):
        unit(0, 0)
    with jax.named_scope("s_u1"):
        for o in (0, 1, 3, 2):
            zz = rem4(z + o)
            landed(k_src.at[0], xr.at[zz])
            x_copy(0, rem4(x + 1), zz, rem4(x - 1), 1, 9).start()
            landed(k_src.at[0], xr.at[4 + zz])
            x_copy(1, rem4(x - 1), zz, rem4(x + 1), 1, 9).start()
        landed(k_all.at[0:2], xr.at[8])
        unit(1, 0)
        unit(3, 0)
        landed(k_all.at[0:2], xr.at[9])
        unit(2, 0)

    def block(i, _):
        soft(i)
        scores(i)
        return 0

    with jax.named_scope("s_b0"):
        lax.fori_loop(0, 2, block, 0)

    def whole_block(i, _):
        whole(i)
        scores(i)
        return 0

    def shard(i, _):
        o = 1 + 2 * i - 3 * (i // 2)
        with jax.named_scope("s_qw"):
            landed(q_all.at[0:2], zr.at[1, rem4(z + o)])
        prepare(o)
        lax.fori_loop(2 * o, 2 * o + 2, whole_block, 0)
        return 0

    with jax.named_scope("s_b1"):
        lax.fori_loop(0, 3, shard, 0)
    k_t[...] = k_all[...].reshape(NSP * T, D).T
    def grads_out(left, right, src, into, which):
        def step(t, _):
            xx = lax.rem(x + 1 + t // 2, NX)
            half = lax.rem(t, 2)
            at = pl.ds(pl.multiple_of(xx * 512 + half * 256, 256), 256)
            out = dot_nn(left[0, at, :], right[0:256, :])
            for j in range(1, 8):
                out = out + dot_nn(left[j, at, :], right[j * 256 : (j + 1) * 256, :])
            for j in range(2):
                src(xx, 2 * half + j)[...] = out[j * T : (j + 1) * T].astype(BF)
            for j in range(2):
                zz = 2 * half + j
                peer = zz * NX + xx

                @pl.when(peer != sp)
                def _():
                    remote(
                        src(xx, zz), into.at[sp], dps.at[which], dpr.at[which], sp=peer
                    ).start()

            return 0

        lax.fori_loop(0, 2 * NX, step, 0)
        into[sp] = src(x, z)[...]

    def wait_grads(into, which):
        landed(into.at[0 : NSP - 1], dpr.at[which])

    def head_sum(into, h):
        total = into[NX * h].astype(F32)
        for xx in range(1, NX):
            total = total + into[NX * h + xx].astype(F32)
        return total

    def along_y(o, slot_y, rows, buf, which):
        peer = rem4(y + o)
        at = buf.at[2 * slot_y + core, rows]
        return remote(at, at, as_.at[which], ar.at[which, slot_y], dp=2 * peer + core)

    def cross(yy, buf, which):
        slot = 2 * yy + core
        return remote(
            buf.at[slot], buf.at[slot], as_.at[which], ar.at[which, 4], dp=2 * y + (1 - core)
        )

    def gather_start(buf, which):
        along_y(1, y, slice(0, T), buf, which).start()
        along_y(3, y, slice(0, T), buf, which).start()
        cross(y, buf, which).start()

    def gather_relay(buf, which):
        for o in (1, 3):
            yy = rem4(y + o)
            landed(buf.at[0], ar.at[which, yy])
            along_y(4 - o, yy, slice(0, 64) if o == 1 else slice(64, T), buf, which).start()
            cross(yy, buf, which).start()

    def gather_last(buf, which):
        yy = rem4(y + 2)
        landed(buf.at[0], ar.at[which, yy])
        cross(yy, buf, which).start()

    def gather_finish(buf, which):
        landed(buf.at[0:4], ar.at[which, 4])

    def gi_src(peer):
        return li_all.at[peer]

    outs = (gwv, gwk)

    def stage_copy(stage, which, half, o):
        along_x = (half == 0) == (stage != 1)
        me = x if along_x else z
        peer = rem4(me + o)
        wide = slice(half * 256, (half + 1) * 256)
        if stage == 0:
            src = pb.at[half, pl.ds(pl.multiple_of(which * 512 + peer * T, T), T)]
            dst = r1.at[which, half, me]
        elif stage == 1:
            src, dst = st1.at[which, half], r2.at[which, half, me]
        else:
            src, dst = go.at[which, half], outs[which].at[cols(me, T), wide]
        target = z * NX + peer if along_x else peer * NX + x
        return remote(src, dst, ts.at[stage], trs.at[stage, which, half], sp=target)

    def stage_start(stage, which, half):
        for o in order:
            stage_copy(stage, which, half, o).start()

    def stage_wait(stage, which, half):
        landed(r1.at[which, half, 0:3], trs.at[stage, which, half])

    def own_part(which, half):
        return pltpu.make_async_copy(
            go.at[which, half],
            outs[which].at[cols(x if half == 0 else z, T), half * 256 : (half + 1) * 256],
            loc.at[12 + 2 * which + half],
        )

    def reduce_start(buf, which):
        out = dot_tn(li_all[...].reshape(NDP * T, 512), buf[...].reshape(NDP * T, 512))
        for half in range(2):
            pb[half, which * 512 : (which + 1) * 512, :] = out[:, half * 256 : (half + 1) * 256].astype(BF)
        for half in range(2):
            stage_start(0, which, half)

    def reduce_first(which):
        for half in range(2):
            me = x if half == 0 else z
            stage_wait(0, which, half)
            at = pl.ds(pl.multiple_of(which * 512 + me * T, T), T)
            total = pb[half, at].astype(F32)
            for o in order:
                total = total + r1[which, half, rem4(me + o)].astype(F32)
            st1[which, half] = total.astype(BF)
            stage_start(1, which, half)

    def reduce_second(which):
        for half in range(2):
            me = z if half == 0 else x
            stage_wait(1, which, half)
            total = st1[which, half].astype(F32)
            for o in order:
                total = total + r2[which, half, rem4(me + o)].astype(F32)
            go[which, half] = total.astype(BF)
            stage_start(2, which, half)
            own_part(which, half).start()

    with jax.named_scope("s_dk"):
        grads_out(ds, qs, lambda xx, zz: dk_src.at[xx, zz], dk_in, 1)

    def query_grads(i):
        off = i // 2
        zz = lax.rem(z + off, NZ)
        pair = lax.rem(i, 2)
        wide = pl.ds(pl.multiple_of(pair * 256, 256), 256)
        grad = dot_nn(k_t[...], ds[i]).T * SCALE
        both = q_all[zz, :, wide].astype(F32)
        outs = []
        for h in range(2):
            outs.append(
                norm_back(
                    grad[h * D : (h + 1) * D], both[:, h * D : (h + 1) * D], qg[...],
                    tab[zz, 0], tab[zz, 1], tab[zz, 2],
                ).astype(BF)
            )
        dq_out[zz, :, wide] = jnp.concatenate(outs, axis=1)

    def query_send(i):
        off = i // 2
        zz = lax.rem(z + off, NZ)
        pair = lax.rem(i, 2)

        if isinstance(i, int):
            if i == 1:
                pltpu.make_async_copy(dq_out.at[z], gq.at[:, cols(z, 512)], loc.at[6]).start()
            else:
                dq_copy(zz).start()
        else:

            @pl.when(pair == 1)
            def _():
                dq_copy(zz).start()

    def back(t, _):
        query_grads(t)

        @pl.when(t >= 4)
        def _():
            query_send(t)

        return 0

    with jax.named_scope("s_dq1"):
        lax.fori_loop(0, 4, back, 0)
    with jax.named_scope("s_dv"):
        grads_out(pb, gs, lambda xx, zz: g_all.at[xx, :, cols(zz, D)], dv_in, 0)
    query_send(1)
    query_send(3)
    with jax.named_scope("s_wdk"):
        wait_grads(dk_in, 1)
    pieces = []
    for h in range(NZ):
        u = k[:, h * D : (h + 1) * D].astype(F32)
        pieces.append(
            norm_back(head_sum(dk_in, h) * SCALE, u, kg[...], tab[z, 0], tab[z, 1], tab[z, 2]).astype(BF)
        )
    ks_all[dp] = jnp.concatenate(pieces, axis=1)
    gather_start(ks_all, 1)

    with jax.named_scope("s_dq2"):
        lax.fori_loop(4, 8, back, 0)
    with jax.named_scope("s_rlk"):
        gather_relay(ks_all, 1)
    with jax.named_scope("s_wdv"):
        wait_grads(dv_in, 0)
    vs_all[dp] = jnp.concatenate([head_sum(dv_in, h).astype(BF) for h in range(NZ)], axis=1)
    gather_start(vs_all, 0)
    own[3].wait()

    landed(li_all.at[0 : NDP - 1], misc.at[1])
    with jax.named_scope("s_gfk"):
        gather_last(ks_all, 1)
        gather_finish(ks_all, 1)
    with jax.named_scope("s_rsk"):
        reduce_start(ks_all, 1)
    with jax.named_scope("s_gfv"):
        gather_relay(vs_all, 0)
        gather_last(vs_all, 0)
        gather_finish(vs_all, 0)
    with jax.named_scope("s_rsv"):
        reduce_start(vs_all, 0)

    with jax.named_scope("s_rf1k"):
        reduce_first(1)

    own[4].wait()
    own[5].wait()

    def gi_copy(peer):
        return remote(gi_src(peer), gin.at[:, cols(dp, 512)], misc.at[4], misc.at[5], dp=peer)

    def grad_in(i, _):
        group = lax.rem(dp // 4 + 1 + i, 2)
        four = pl.ds(4 * group, 4)
        out = dot_nt(ks_all[four].reshape(512, 512), kw_s[...])
        out = out + dot_nt(vs_all[four].reshape(512, 512), vw_s[...])
        li_all[four] = out.astype(BF).reshape(4, T, 512)
        for j in range(4):
            peer = 4 * group + j

            @pl.when(peer != dp)
            def _():
                gi_copy(peer).start()

        return 0

    with jax.named_scope("s_gin"):
        lax.fori_loop(0, 2, grad_in, 0)
    pltpu.make_async_copy(gi_src(dp), gin.at[:, cols(dp, 512)], loc.at[16]).start()

    with jax.named_scope("s_rf1v"):
        reduce_first(0)
    with jax.named_scope("s_rf2"):
        reduce_second(1)
        reduce_second(0)
    sent(k_src.at[0:3], zs.at[0])
    sent(k_src.at[0:3], zs.at[1])
    sent(q_all.at[0:3], zs.at[2])
    sent(q_all.at[0:3], zs.at[3])
    sent(k_all, xs.at[0])
    sent(k_all.at[0:2], xs.at[1])
    sent(li_all.at[0 : NDP - 1], misc.at[0])
    sent(dq_out.at[0:3], misc.at[2])
    landed(dq_out.at[0:3], misc.at[3])
    for which, buf in ((0, vs_all), (1, ks_all)):
        sent(dv_in.at[0 : NSP - 1], dps.at[which])
        sent(buf.at[0 : NDP - 1], as_.at[which])
    pltpu.make_async_copy(dq_out.at[z], gq.at[:, cols(z, 512)], loc.at[6]).wait()
    pltpu.make_async_copy(gi_src(dp), gin.at[:, cols(dp, 512)], loc.at[16]).wait()
    with jax.named_scope("s_drdp"):
        sent(li_all.at[0 : NDP - 1], misc.at[4])
        landed(li_all.at[0 : NDP - 1], misc.at[5])
    with jax.named_scope("s_drsp"):
        for which in (1, 0):
            for half in range(2):
                stage_wait(2, which, half)
                own_part(which, half).wait()
        for stage in range(3):
            sent(r1.at[:, :, 0:3], ts.at[stage])


def finish(gq_in, gin_in, gwv_in, gwk_in, gq, gin, gwv, gwk, a, b, c, e, sem):
    ins, outs = [], []
    for i in range(4):
        at = slice(i * 32, (i + 1) * 32)
        rows = slice(i * T, (i + 1) * T)
        ins.append(
            [
                pltpu.make_async_copy(gwk_in.at[rows], c.at[0, rows], sem.at[0, i, 0]),
                pltpu.make_async_copy(gwv_in.at[rows], c.at[1, rows], sem.at[0, i, 1]),
                pltpu.make_async_copy(gin_in.at[at], b.at[at], sem.at[0, i, 2]),
                pltpu.make_async_copy(gq_in.at[at], a.at[at], sem.at[0, i, 3]),
            ]
        )
        outs.append(
            [
                pltpu.make_async_copy(e.at[0, rows], gwk.at[rows], sem.at[1, i, 0]),
                pltpu.make_async_copy(e.at[1, rows], gwv.at[rows], sem.at[1, i, 1]),
                pltpu.make_async_copy(b.at[at], gin.at[at], sem.at[1, i, 2]),
                pltpu.make_async_copy(a.at[at], gq.at[at], sem.at[1, i, 3]),
            ]
        )
    for group in ins:
        for copy in group:
            copy.start()
    for i in range(4):
        rows = slice(i * T, (i + 1) * T)
        for j in range(4):
            ins[i][j].wait()
            if j < 2:
                e[j, rows] = c[j, rows].astype(F32)
            outs[i][j].start()
    for group in outs:
        for copy in group:
            copy.wait()


def on_device(queries, keys, values, out_grad, layer_in, key_weight, value_weight, query_gain, key_gain):
    rows, cols = rope_tables()
    hbm = pl.BlockSpec(memory_space=pl.ANY)
    dma = pltpu.SemaphoreType.DMA
    V = pltpu.VMEM
    gq, gin, gwv, gwk = pl.pallas_call(
        body,
        out_shape=(
            jax.ShapeDtypeStruct((T, 2048), BF),
            jax.ShapeDtypeStruct((T, 4096), BF),
            jax.ShapeDtypeStruct((512, 512), BF),
            jax.ShapeDtypeStruct((512, 512), BF),
        ),
        in_specs=[hbm] * 11,
        out_specs=(hbm, hbm, hbm, hbm),
        scratch_shapes=[
            V((T, 512), BF),
            V((1, D), F32),
            V((1, D), F32),
            V(rows.shape, F32),
            V(cols.shape, F32),
            V((NZ, T, 512), BF),
            V((NZ, T, 512), BF),
            V((NX, NZ, T, D), BF),
            V((NX, NZ, T, D), BF),
            V((NZ, T, D), BF),
            V((D, 2048), BF),
            V((NZ, 3, T, D), F32),
            V((2048, D), BF),
            V((2048, D), BF),
            V((8, 2048), F32),
            V((8, 2048), F32),
            V((8, 2048), F32),
            V((8, 2048, 256), F32),
            V((8, 2048, 256), F32),
            V((8, 2048, 256), BF),
            V((8, 2048, 256), BF),
            V((NZ, T, 512), BF),
            V((NX, NZ, T, D), BF),
            V((NSP, T, D), BF),
            V((NSP, T, D), BF),
            V((NDP, T, 512), BF),
            V((512, 512), BF),
            V((512, 512), BF),
            V((NDP, T, 512), BF),
            V((NDP, T, 512), BF),
            V((2, 2, 4, T, 256), BF),
            V((2, 2, T, 256), BF),
            V((2, 2, 4, T, 256), BF),
            V((2, 2, T, 256), BF),
            dma((17,)),
            dma((4,)),
            dma((2, NZ)),
            dma((2,)),
            dma((10,)),
            dma((6,)),
            dma((2,)),
            dma((2,)),
            dma((2,)),
            dma((2, 5)),
            dma((3,)),
            dma((3, 2, 2)),
        ],
        compiler_params=pltpu.CompilerParams(
            collective_id=0, has_side_effects=True, vmem_limit_bytes=67043328
        ),
        name="step",
    )(
        queries[0], keys[0], values[0], out_grad[0], layer_in[0], key_weight, value_weight,
        query_gain.reshape(1, D), key_gain.reshape(1, D), jnp.asarray(rows), jnp.asarray(cols),
    )
    gq, gin, gwv, gwk = pl.pallas_call(
        finish,
        out_shape=(
            jax.ShapeDtypeStruct((T, 2048), BF),
            jax.ShapeDtypeStruct((T, 4096), BF),
            jax.ShapeDtypeStruct((512, 512), F32),
            jax.ShapeDtypeStruct((512, 512), F32),
        ),
        in_specs=[hbm] * 4,
        out_specs=(hbm,) * 4,
        scratch_shapes=[
            V((T, 2048), BF),
            V((T, 4096), BF),
            V((2, 512, 512), BF),
            V((2, 512, 512), F32),
            dma((2, 4, 4)),
        ],
        name="finish",
    )(gq, gin, gwv, gwk)
    return gq[None], gin[None], gwk, gwv


def solution(mesh):
    in_specs = (
        P("dp", "sp", None),
        P("dp", "sp", None),
        P("dp", "sp", None),
        P("dp", "sp", None),
        P("dp", "sp", None),
        P("dp", None),
        P("dp", None),
        P(),
        P(),
    )
    out_specs = (P("dp", "sp", None), P("dp", "sp", None), P("dp", None), P("dp", None))
    return jax.shard_map(
        on_device, mesh=mesh, in_specs=in_specs, out_specs=out_specs, check_vma=False
    )
```

```python
import functools

import jax
import jax.numpy as jnp
import numpy as np
from jax import lax
from jax.experimental import pallas as pl
from jax.experimental.pallas import tpu as pltpu
from jax.sharding import PartitionSpec as P

D = 128
GRID_W = 64
EPS = 1e-6
BASE = 10000.0
NZ = 4
NX = 4
NY = 4
NSP = NZ * NX
NDP = 2 * NY
T = 128
KC = 64
BF = jnp.bfloat16
F32 = jnp.float32
SCALE = D ** -0.5
EXP2_SCALE = float(SCALE * np.log2(np.e))


def rope_tables():
    quarter = D // 4
    inverse = np.float32(BASE) ** (-np.arange(quarter, dtype=np.float32) / np.float32(quarter))

    def one(count, half):
        angles = np.arange(count, dtype=np.float32)[:, None] * inverse[None, :]
        cosine, sine = np.cos(angles), np.sin(angles)
        table = np.zeros((3, count, D), np.float32)
        lo = half * 2 * quarter
        table[0, :, lo : lo + quarter] = cosine
        table[0, :, lo + quarter : lo + 2 * quarter] = cosine
        table[1, :, lo + quarter : lo + 2 * quarter] = sine
        table[2, :, lo : lo + quarter] = -sine
        return table

    rows = one(2048 // GRID_W, 0).reshape(3, 2048 // GRID_W, 1, D)
    cols = one(GRID_W, 1)
    return rows, cols


def rotate(n, c, s1, s2):
    return n * c + pltpu.roll(n, 32, 1) * s1 + pltpu.roll(n, 96, 1) * s2


def unrotate(n, c, s1, s2):
    return n * c - pltpu.roll(n, 32, 1) * s1 - pltpu.roll(n, 96, 1) * s2


def inv_rms(u):
    return lax.rsqrt(jnp.mean(u * u, axis=1, keepdims=True) + EPS)


def norm_back(grad, u, gain, c, s1, s2):
    r = inv_rms(u)
    t = unrotate(grad, c, s1, s2) * gain
    dot = jnp.sum(t * u, axis=1, keepdims=True)
    return r * t - u * (r * r * r * (1.0 / D) * dot)


def dot_nt(a, b):
    return lax.dot_general(a, b, (((1,), (1,)), ((), ())), preferred_element_type=F32)


def dot_nn(a, b):
    return lax.dot_general(a, b, (((1,), (0,)), ((), ())), preferred_element_type=F32)


def dot_tn(a, b):
    return lax.dot_general(a, b, (((0,), (0,)), ((), ())), preferred_element_type=F32)


def body(
    q, k_in, v, g, li, kw, vw, qg_in, kg_in, tr_in, tc_in,
    gq, gin, gwv, gwk,
    k, qg, kg, tr, tc, q_all, g_all, k_all, v_all, k_src, k_t, tab, qs, gs, m_scr, rl_scr, d_scr, s_all, dp_all, pb, ds,
    dq_out, dk_src, dv_in, dk_in, li_all, kw_s, vw_s, vs_all, ks_all,
    r1, st1, r2, go,
    loc, zs, zr, xs, xr, misc, dps, dpr, as_, ar, ts, trs,
):
    sp = lax.axis_index("sp")
    dp = lax.axis_index("dp")
    z, x = sp // NX, lax.rem(sp, NX)
    y, core = dp // 2, lax.rem(dp, 2)

    def remote(src, dst, ss, rs, **where):
        return pltpu.make_async_remote_copy(
            src_ref=src, dst_ref=dst, send_sem=ss, recv_sem=rs,
            device_id=where, device_id_type=pl.DeviceIdType.MESH,
        )

    def sent(ref, sem):
        remote(ref, ref, sem, sem, sp=sp).wait_send()

    def landed(ref, sem):
        remote(ref, ref, sem, sem, sp=sp).wait_recv()

    barrier = pltpu.get_barrier_semaphore()

    def greet_sp(o, _):
        pl.semaphore_signal(
            barrier, inc=1, device_id={"sp": lax.rem(sp + o, NSP)},
            device_id_type=pl.DeviceIdType.MESH,
        )
        return 0

    def greet_dp(o, _):
        pl.semaphore_signal(
            barrier, inc=1, device_id={"dp": lax.rem(dp + o, NDP)},
            device_id_type=pl.DeviceIdType.MESH,
        )
        return 0

    lax.fori_loop(1, NSP, greet_sp, 0)
    lax.fori_loop(1, NDP, greet_dp, 0)

    def cols(i, w):
        return pl.ds(pl.multiple_of(i * w, w), w)

    small = [
        pltpu.make_async_copy(src, dst, loc.at[7 + i])
        for i, (src, dst) in enumerate(
            ((k_in, k), (qg_in, qg), (kg_in, kg), (tr_in, tr), (tc_in, tc))
        )
    ]
    for c in small:
        c.start()
    own = [
        pltpu.make_async_copy(q.at[:, cols(z, 512)], q_all.at[z], loc.at[0]),
        pltpu.make_async_copy(g.at[:, cols(z, 512)], g_all.at[z], loc.at[1]),
        pltpu.make_async_copy(v.at[:, cols(z, D)], v_all.at[x, z], loc.at[2]),
        pltpu.make_async_copy(li.at[:, cols(dp, 512)], li_all.at[dp], loc.at[3]),
        pltpu.make_async_copy(kw, kw_s, loc.at[4]),
        pltpu.make_async_copy(vw, vw_s, loc.at[5]),
    ]
    for c in own:
        c.start()
    for c in small:
        c.wait()

    for zz in range(NZ):
        shard = NX * zz + x
        for kind in range(3):
            part = tc[kind]
            tab[zz, kind, 0:64] = part + tr[kind, 2 * shard]
            tab[zz, kind, 64:128] = part + tr[kind, 2 * shard + 1]

    for h in range(NZ):
        u = k[:, h * D : (h + 1) * D].astype(F32)
        n = u * inv_rms(u) * kg[...]
        k_src[h] = rotate(n, tab[z, 0], tab[z, 1], tab[z, 2]).astype(BF)
    k_all[x, z] = k_src[z]

    with jax.named_scope("s_barrier"):
        pl.semaphore_wait(barrier, NSP + NDP - 2)

    def z_copies(o, side, kinds):
        peer = lax.rem(z + o, NZ)
        slot = z if side == "send" else peer
        pairs = (
            (k_src.at[peer], k_all.at[x, slot]),
            (v.at[:, cols(peer, D)], v_all.at[x, slot]),
            (q.at[:, cols(peer, 512)], q_all.at[slot]),
            (g.at[:, cols(peer, 512)], g_all.at[slot]),
        )
        return [
            remote(*pairs[i], zs.at[i], zr.at[i // 2, slot], sp=peer * NX + x) for i in kinds
        ]

    order = (1, 3, 2)
    own[2].wait()
    for o in order:
        for c in z_copies(o, "send", (0, 1)):
            c.start()

    kv = (k_all, v_all)

    def rem4(i):
        return lax.rem(i + 4, 4)

    def x_copy(kind, chunk, zz, peer, ss, rs):
        at = kv[kind].at[chunk, zz]
        return remote(at, at, xs.at[ss], xr.at[rs], sp=z * NX + peer)

    def x_send(zz):
        x_copy(0, x, zz, rem4(x - 1), 0, zz).start()
        x_copy(1, x, zz, rem4(x + 1), 0, 4 + zz).start()
        x_copy(0, x, zz, rem4(x + 1), 0, 8).start()
        x_copy(1, x, zz, rem4(x - 1), 0, 8).start()

    x_send(z)
    for o in (1, 3):
        for c in z_copies(o, "send", (2, 3)):
            c.start()

    def li_copy(o, side):
        peer = lax.rem(dp + o, NDP)
        slot = dp if side == "send" else peer
        return remote(li.at[:, cols(peer, 512)], li_all.at[slot], misc.at[0], misc.at[1], dp=peer)

    def li_start(o, _):
        li_copy(o, "send").start()
        return 0

    lax.fori_loop(1, NDP, li_start, 0)

    def dq_copy(zz):
        return remote(dq_out.at[zz], gq.at[:, cols(z, 512)], misc.at[2], misc.at[3], sp=zz * NX + x)

    def prepare(o):
        zz = lax.rem(z + o, NZ)
        for h in range(4):
            rows = pl.ds(pl.multiple_of(o * 512 + h * T, T), T)
            u = q_all[zz, :, h * D : (h + 1) * D].astype(F32)
            n = u * inv_rms(u) * qg[...]
            qs[rows, :] = rotate(n, tab[zz, 0], tab[zz, 1], tab[zz, 2]).astype(BF)
            gs[rows, :] = g_all[zz, :, h * D : (h + 1) * D]

    def unit(xo, o):
        xx = lax.rem(x + xo, NX)
        qcols = pl.ds(pl.multiple_of(o * 512, 512), 512)
        qb, gb = qs[qcols, :], gs[qcols, :]
        for half in range(2):
            kc = k_all[xx, 2 * half : 2 * half + 2].reshape(256, D)
            vc = v_all[xx, 2 * half : 2 * half + 2].reshape(256, D)
            rows = pl.ds(pl.multiple_of(xx * 512 + half * 256, 256), 256)
            s = dot_nt(kc, qb)
            s_all[2 * o, rows, :] = s[:, :256]
            s_all[2 * o + 1, rows, :] = s[:, 256:]
            m_scr[:, qcols] = jnp.maximum(m_scr[:, qcols], jnp.max(s.reshape(32, 8, 512), axis=0))
            w = dot_nt(vc, gb)
            dp_all[2 * o, rows, :] = w[:, :256]
            dp_all[2 * o + 1, rows, :] = w[:, 256:]

    m_scr[...] = jnp.full((8, 2048), -jnp.inf, F32)
    own[0].wait()
    own[1].wait()
    def block_cols(i):
        return pl.ds(pl.multiple_of(i * 256, 256), 256)

    def exps(i, j, m, l8):
        at = slice(j * KC, (j + 1) * KC)
        e = jnp.exp2(s_all[i, at, :] * EXP2_SCALE - m)
        s_all[i, at, :] = e
        return l8 + jnp.sum(e.reshape(KC // 8, 8, 256), axis=0)

    def soft(i):
        m = jnp.max(m_scr[:, block_cols(i)], axis=0, keepdims=True) * EXP2_SCALE
        l8 = jnp.zeros((8, 256), F32)
        for j in range(2048 // KC):
            l8 = exps(i, j, m, l8)
        probs(i, l8)

    def whole(i):
        rows = pl.ds(pl.multiple_of(i * 256, 256), 256)
        qb, gb = qs[rows, :], gs[rows, :]
        m8 = jnp.full((8, 256), -jnp.inf, F32)
        for j in range(NX):
            s = dot_nt(k_all[j].reshape(512, D), qb)
            s_all[i, j * 512 : (j + 1) * 512, :] = s
            m8 = jnp.maximum(m8, jnp.max(s.reshape(64, 8, 256), axis=0))
        m = jnp.max(m8, axis=0, keepdims=True) * EXP2_SCALE
        l8 = jnp.zeros((8, 256), F32)
        for j in range(2 * NX):
            vb = v_all[j // 2, 2 * (j % 2) : 2 * (j % 2) + 2].reshape(256, D)
            dp_all[i, j * 256 : (j + 1) * 256, :] = dot_nt(vb, gb)
            for n in range(4):
                l8 = exps(i, 4 * j + n, m, l8)
        probs(i, l8)

    def probs(i, l8):
        here = block_cols(i)
        rl = 1.0 / jnp.sum(l8, axis=0, keepdims=True)
        rl_scr[:, here] = jnp.broadcast_to(rl, (8, 256))
        d8 = jnp.zeros((8, 256), F32)
        for j in range(2048 // KC):
            at = slice(j * KC, (j + 1) * KC)
            p_b = (s_all[i, at, :] * rl).astype(BF)
            pb[i, at, :] = p_b
            prod = p_b.astype(F32) * dp_all[i, at, :]
            d8 = d8 + jnp.sum(prod.reshape(KC // 8, 8, 256), axis=0)
        d_scr[:, here] = d8

    def scores(i):
        here = block_cols(i)
        delta = jnp.sum(d_scr[:, here], axis=0, keepdims=True)
        rl = rl_scr[0:1, here]
        for j in range(2048 // KC):
            at = slice(j * KC, (j + 1) * KC)
            ds[i, at, :] = ((s_all[i, at, :] * rl) * (dp_all[i, at, :] - delta)).astype(BF)

    prepare(0)
    with jax.named_scope("s_zkv"):
        for o in order:
            landed(k_src.at[0:2], zr.at[0, rem4(z + o)])
            x_send(rem4(z + o))
        for c in z_copies(2, "send", (2, 3)):
            c.start()
    with jax.named_scope("s_u0"):
        unit(0, 0)
    with jax.named_scope("s_u1"):
        for o in (0, 1, 3, 2):
            zz = rem4(z + o)
            landed(k_src.at[0], xr.at[zz])
            x_copy(0, rem4(x + 1), zz, rem4(x - 1), 1, 9).start()
            landed(k_src.at[0], xr.at[4 + zz])
            x_copy(1, rem4(x - 1), zz, rem4(x + 1), 1, 9).start()
        landed(k_all.at[0:2], xr.at[8])
        unit(1, 0)
        unit(3, 0)
        landed(k_all.at[0:2], xr.at[9])
        unit(2, 0)

    def block(i, _):
        soft(i)
        scores(i)
        return 0

    with jax.named_scope("s_b0"):
        lax.fori_loop(0, 2, block, 0)

    def whole_block(i, _):
        whole(i)
        scores(i)
        return 0

    def shard(i, _):
        o = 1 + 2 * i - 3 * (i // 2)
        with jax.named_scope("s_qw"):
            landed(q_all.at[0:2], zr.at[1, rem4(z + o)])
        prepare(o)
        lax.fori_loop(2 * o, 2 * o + 2, whole_block, 0)
        return 0

    with jax.named_scope("s_b1"):
        lax.fori_loop(0, 3, shard, 0)
    k_t[...] = k_all[...].reshape(NSP * T, D).T
    def grads_out(left, right, src, into, which):
        def step(t, _):
            xx = lax.rem(x + 1 + t // 2, NX)
            half = lax.rem(t, 2)
            at = pl.ds(pl.multiple_of(xx * 512 + half * 256, 256), 256)
            out = dot_nn(left[0, at, :], right[0:256, :])
            for j in range(1, 8):
                out = out + dot_nn(left[j, at, :], right[j * 256 : (j + 1) * 256, :])
            for j in range(2):
                src(xx, 2 * half + j)[...] = out[j * T : (j + 1) * T].astype(BF)
            for j in range(2):
                zz = 2 * half + j
                peer = zz * NX + xx

                @pl.when(peer != sp)
                def _():
                    remote(
                        src(xx, zz), into.at[sp], dps.at[which], dpr.at[which], sp=peer
                    ).start()

            return 0

        lax.fori_loop(0, 2 * NX, step, 0)
        into[sp] = src(x, z)[...]

    def wait_grads(into, which):
        landed(into.at[0 : NSP - 1], dpr.at[which])

    def head_sum(into, h):
        total = into[NX * h].astype(F32)
        for xx in range(1, NX):
            total = total + into[NX * h + xx].astype(F32)
        return total

    def along_y(o, slot_y, rows, buf, which):
        peer = rem4(y + o)
        at = buf.at[2 * slot_y + core, rows]
        return remote(at, at, as_.at[which], ar.at[which, slot_y], dp=2 * peer + core)

    def cross(yy, buf, which):
        slot = 2 * yy + core
        return remote(
            buf.at[slot], buf.at[slot], as_.at[which], ar.at[which, 4], dp=2 * y + (1 - core)
        )

    def gather_start(buf, which):
        along_y(1, y, slice(0, T), buf, which).start()
        along_y(3, y, slice(0, T), buf, which).start()
        cross(y, buf, which).start()

    def gather_relay(buf, which):
        for o in (1, 3):
            yy = rem4(y + o)
            landed(buf.at[0], ar.at[which, yy])
            along_y(4 - o, yy, slice(0, 64) if o == 1 else slice(64, T), buf, which).start()
            cross(yy, buf, which).start()

    def gather_last(buf, which):
        yy = rem4(y + 2)
        landed(buf.at[0], ar.at[which, yy])
        cross(yy, buf, which).start()

    def gather_finish(buf, which):
        landed(buf.at[0:4], ar.at[which, 4])

    def gi_src(peer):
        return li_all.at[peer]

    outs = (gwv, gwk)

    def stage_copy(stage, which, half, o):
        along_x = (half == 0) == (stage != 1)
        me = x if along_x else z
        peer = rem4(me + o)
        wide = slice(half * 256, (half + 1) * 256)
        if stage == 0:
            src = pb.at[half, pl.ds(pl.multiple_of(which * 512 + peer * T, T), T)]
            dst = r1.at[which, half, me]
        elif stage == 1:
            src, dst = st1.at[which, half], r2.at[which, half, me]
        else:
            src, dst = go.at[which, half], outs[which].at[cols(me, T), wide]
        target = z * NX + peer if along_x else peer * NX + x
        return remote(src, dst, ts.at[stage], trs.at[stage, which, half], sp=target)

    def stage_start(stage, which, half):
        for o in (2, 1, 3):
            stage_copy(stage, which, half, o).start()

    def stage_wait(stage, which, half):
        landed(r1.at[which, half, 0:3], trs.at[stage, which, half])

    def own_part(which, half):
        return pltpu.make_async_copy(
            go.at[which, half],
            outs[which].at[cols(x if half == 0 else z, T), half * 256 : (half + 1) * 256],
            loc.at[12 + 2 * which + half],
        )

    def reduce_start(buf, which):
        out = dot_tn(li_all[...].reshape(NDP * T, 512), buf[...].reshape(NDP * T, 512))
        for half in range(2):
            pb[half, which * 512 : (which + 1) * 512, :] = out[:, half * 256 : (half + 1) * 256].astype(BF)
        for half in range(2):
            stage_start(0, which, half)

    def reduce_first(which):
        for half in range(2):
            me = x if half == 0 else z
            stage_wait(0, which, half)
            at = pl.ds(pl.multiple_of(which * 512 + me * T, T), T)
            total = pb[half, at].astype(F32)
            for o in order:
                total = total + r1[which, half, rem4(me + o)].astype(F32)
            st1[which, half] = total.astype(BF)
            stage_start(1, which, half)

    def reduce_second(which):
        for half in range(2):
            me = z if half == 0 else x
            stage_wait(1, which, half)
            total = st1[which, half].astype(F32)
            for o in order:
                total = total + r2[which, half, rem4(me + o)].astype(F32)
            go[which, half] = total.astype(BF)
            stage_start(2, which, half)
            own_part(which, half).start()

    with jax.named_scope("s_dk"):
        grads_out(ds, qs, lambda xx, zz: dk_src.at[xx, zz], dk_in, 1)

    def query_grads(i):
        off = i // 2
        zz = lax.rem(z + off, NZ)
        pair = lax.rem(i, 2)
        wide = pl.ds(pl.multiple_of(pair * 256, 256), 256)
        grad = dot_nn(k_t[...], ds[i]).T * SCALE
        both = q_all[zz, :, wide].astype(F32)
        outs = []
        for h in range(2):
            outs.append(
                norm_back(
                    grad[h * D : (h + 1) * D], both[:, h * D : (h + 1) * D], qg[...],
                    tab[zz, 0], tab[zz, 1], tab[zz, 2],
                ).astype(BF)
            )
        dq_out[zz, :, wide] = jnp.concatenate(outs, axis=1)

    def query_send(i):
        off = i // 2
        zz = lax.rem(z + off, NZ)
        pair = lax.rem(i, 2)

        if isinstance(i, int):
            if i == 1:
                pltpu.make_async_copy(dq_out.at[z], gq.at[:, cols(z, 512)], loc.at[6]).start()
            else:
                dq_copy(zz).start()
        else:

            @pl.when(pair == 1)
            def _():
                dq_copy(zz).start()

    def back(t, _):
        query_grads(t)

        @pl.when(t >= 4)
        def _():
            query_send(t)

        return 0

    with jax.named_scope("s_dq1"):
        lax.fori_loop(0, 4, back, 0)
    with jax.named_scope("s_dv"):
        grads_out(pb, gs, lambda xx, zz: g_all.at[xx, :, cols(zz, D)], dv_in, 0)
    query_send(1)
    query_send(3)
    with jax.named_scope("s_wdk"):
        wait_grads(dk_in, 1)
    pieces = []
    for h in range(NZ):
        u = k[:, h * D : (h + 1) * D].astype(F32)
        pieces.append(
            norm_back(head_sum(dk_in, h) * SCALE, u, kg[...], tab[z, 0], tab[z, 1], tab[z, 2]).astype(BF)
        )
    ks_all[dp] = jnp.concatenate(pieces, axis=1)
    gather_start(ks_all, 1)

    with jax.named_scope("s_dq2"):
        lax.fori_loop(4, 8, back, 0)
    with jax.named_scope("s_rlk"):
        gather_relay(ks_all, 1)
    with jax.named_scope("s_wdv"):
        wait_grads(dv_in, 0)
    vs_all[dp] = jnp.concatenate([head_sum(dv_in, h).astype(BF) for h in range(NZ)], axis=1)
    gather_start(vs_all, 0)
    own[3].wait()

    landed(li_all.at[0 : NDP - 1], misc.at[1])
    with jax.named_scope("s_gfk"):
        gather_last(ks_all, 1)
        gather_finish(ks_all, 1)
    with jax.named_scope("s_rsk"):
        reduce_start(ks_all, 1)
    with jax.named_scope("s_gfv"):
        gather_relay(vs_all, 0)
        gather_last(vs_all, 0)
        gather_finish(vs_all, 0)
    with jax.named_scope("s_rsv"):
        reduce_start(vs_all, 0)

    with jax.named_scope("s_rf1k"):
        reduce_first(1)

    own[4].wait()
    own[5].wait()

    def gi_copy(peer):
        return remote(gi_src(peer), gin.at[:, cols(dp, 512)], misc.at[4], misc.at[5], dp=peer)

    def grad_in(i, _):
        group = lax.rem(dp // 4 + 1 + i, 2)
        four = pl.ds(4 * group, 4)
        out = dot_nt(ks_all[four].reshape(512, 512), kw_s[...])
        out = out + dot_nt(vs_all[four].reshape(512, 512), vw_s[...])
        li_all[four] = out.astype(BF).reshape(4, T, 512)
        for j in range(4):
            peer = 4 * group + j

            @pl.when(peer != dp)
            def _():
                gi_copy(peer).start()

        return 0

    with jax.named_scope("s_gin"):
        lax.fori_loop(0, 2, grad_in, 0)
    pltpu.make_async_copy(gi_src(dp), gin.at[:, cols(dp, 512)], loc.at[16]).start()

    with jax.named_scope("s_rf1v"):
        reduce_first(0)
    with jax.named_scope("s_rf2"):
        reduce_second(1)
        reduce_second(0)
    sent(k_src.at[0:3], zs.at[0])
    sent(k_src.at[0:3], zs.at[1])
    sent(q_all.at[0:3], zs.at[2])
    sent(q_all.at[0:3], zs.at[3])
    sent(k_all, xs.at[0])
    sent(k_all.at[0:2], xs.at[1])
    sent(li_all.at[0 : NDP - 1], misc.at[0])
    sent(dq_out.at[0:3], misc.at[2])
    landed(dq_out.at[0:3], misc.at[3])
    for which, buf in ((0, vs_all), (1, ks_all)):
        sent(dv_in.at[0 : NSP - 1], dps.at[which])
        sent(buf.at[0 : NDP - 1], as_.at[which])
    pltpu.make_async_copy(dq_out.at[z], gq.at[:, cols(z, 512)], loc.at[6]).wait()
    pltpu.make_async_copy(gi_src(dp), gin.at[:, cols(dp, 512)], loc.at[16]).wait()
    with jax.named_scope("s_drdp"):
        sent(li_all.at[0 : NDP - 1], misc.at[4])
        landed(li_all.at[0 : NDP - 1], misc.at[5])
    with jax.named_scope("s_drsp"):
        for which in (1, 0):
            for half in range(2):
                stage_wait(2, which, half)
                own_part(which, half).wait()
        for stage in range(3):
            sent(r1.at[:, :, 0:3], ts.at[stage])


def finish(gq_in, gin_in, gwv_in, gwk_in, gq, gin, gwv, gwk, a, b, c, e, sem):
    ins, outs = [], []
    for i in range(4):
        at = slice(i * 32, (i + 1) * 32)
        rows = slice(i * T, (i + 1) * T)
        ins.append(
            [
                pltpu.make_async_copy(gwk_in.at[rows], c.at[0, rows], sem.at[0, i, 0]),
                pltpu.make_async_copy(gwv_in.at[rows], c.at[1, rows], sem.at[0, i, 1]),
                pltpu.make_async_copy(gin_in.at[at], b.at[at], sem.at[0, i, 2]),
                pltpu.make_async_copy(gq_in.at[at], a.at[at], sem.at[0, i, 3]),
            ]
        )
        outs.append(
            [
                pltpu.make_async_copy(e.at[0, rows], gwk.at[rows], sem.at[1, i, 0]),
                pltpu.make_async_copy(e.at[1, rows], gwv.at[rows], sem.at[1, i, 1]),
                pltpu.make_async_copy(b.at[at], gin.at[at], sem.at[1, i, 2]),
                pltpu.make_async_copy(a.at[at], gq.at[at], sem.at[1, i, 3]),
            ]
        )
    for group in ins:
        for copy in group:
            copy.start()
    for i in range(4):
        rows = slice(i * T, (i + 1) * T)
        for j in range(4):
            ins[i][j].wait()
            if j < 2:
                e[j, rows] = c[j, rows].astype(F32)
            outs[i][j].start()
    for group in outs:
        for copy in group:
            copy.wait()


def on_device(queries, keys, values, out_grad, layer_in, key_weight, value_weight, query_gain, key_gain):
    rows, cols = rope_tables()
    hbm = pl.BlockSpec(memory_space=pl.ANY)
    dma = pltpu.SemaphoreType.DMA
    V = pltpu.VMEM
    gq, gin, gwv, gwk = pl.pallas_call(
        body,
        out_shape=(
            jax.ShapeDtypeStruct((T, 2048), BF),
            jax.ShapeDtypeStruct((T, 4096), BF),
            jax.ShapeDtypeStruct((512, 512), BF),
            jax.ShapeDtypeStruct((512, 512), BF),
        ),
        in_specs=[hbm] * 11,
        out_specs=(hbm, hbm, hbm, hbm),
        scratch_shapes=[
            V((T, 512), BF),
            V((1, D), F32),
            V((1, D), F32),
            V(rows.shape, F32),
            V(cols.shape, F32),
            V((NZ, T, 512), BF),
            V((NZ, T, 512), BF),
            V((NX, NZ, T, D), BF),
            V((NX, NZ, T, D), BF),
            V((NZ, T, D), BF),
            V((D, 2048), BF),
            V((NZ, 3, T, D), F32),
            V((2048, D), BF),
            V((2048, D), BF),
            V((8, 2048), F32),
            V((8, 2048), F32),
            V((8, 2048), F32),
            V((8, 2048, 256), F32),
            V((8, 2048, 256), F32),
            V((8, 2048, 256), BF),
            V((8, 2048, 256), BF),
            V((NZ, T, 512), BF),
            V((NX, NZ, T, D), BF),
            V((NSP, T, D), BF),
            V((NSP, T, D), BF),
            V((NDP, T, 512), BF),
            V((512, 512), BF),
            V((512, 512), BF),
            V((NDP, T, 512), BF),
            V((NDP, T, 512), BF),
            V((2, 2, 4, T, 256), BF),
            V((2, 2, T, 256), BF),
            V((2, 2, 4, T, 256), BF),
            V((2, 2, T, 256), BF),
            dma((17,)),
            dma((4,)),
            dma((2, NZ)),
            dma((2,)),
            dma((10,)),
            dma((6,)),
            dma((2,)),
            dma((2,)),
            dma((2,)),
            dma((2, 5)),
            dma((3,)),
            dma((3, 2, 2)),
        ],
        compiler_params=pltpu.CompilerParams(
            collective_id=0, has_side_effects=True, vmem_limit_bytes=67043328
        ),
        name="step",
    )(
        queries[0], keys[0], values[0], out_grad[0], layer_in[0], key_weight, value_weight,
        query_gain.reshape(1, D), key_gain.reshape(1, D), jnp.asarray(rows), jnp.asarray(cols),
    )
    gq, gin, gwv, gwk = pl.pallas_call(
        finish,
        out_shape=(
            jax.ShapeDtypeStruct((T, 2048), BF),
            jax.ShapeDtypeStruct((T, 4096), BF),
            jax.ShapeDtypeStruct((512, 512), F32),
            jax.ShapeDtypeStruct((512, 512), F32),
        ),
        in_specs=[hbm] * 4,
        out_specs=(hbm,) * 4,
        scratch_shapes=[
            V((T, 2048), BF),
            V((T, 4096), BF),
            V((2, 512, 512), BF),
            V((2, 512, 512), F32),
            dma((2, 4, 4)),
        ],
        name="finish",
    )(gq, gin, gwv, gwk)
    return gq[None], gin[None], gwk, gwv


def solution(mesh):
    in_specs = (
        P("dp", "sp", None),
        P("dp", "sp", None),
        P("dp", "sp", None),
        P("dp", "sp", None),
        P("dp", "sp", None),
        P("dp", None),
        P("dp", None),
        P(),
        P(),
    )
    out_specs = (P("dp", "sp", None), P("dp", "sp", None), P("dp", None), P("dp", None))
    return jax.shard_map(
        on_device, mesh=mesh, in_specs=in_specs, out_specs=out_specs, check_vma=False
    )
```

```python
import functools

import jax
import jax.numpy as jnp
import numpy as np
from jax import lax
from jax.experimental import pallas as pl
from jax.experimental.pallas import tpu as pltpu
from jax.sharding import PartitionSpec as P

D = 128
GRID_W = 64
EPS = 1e-6
BASE = 10000.0
NZ = 4
NX = 4
NY = 4
NSP = NZ * NX
NDP = 2 * NY
T = 128
KC = 64
BF = jnp.bfloat16
F32 = jnp.float32
SCALE = D ** -0.5
EXP2_SCALE = float(SCALE * np.log2(np.e))


def rope_tables():
    quarter = D // 4
    inverse = np.float32(BASE) ** (-np.arange(quarter, dtype=np.float32) / np.float32(quarter))

    def one(count, half):
        angles = np.arange(count, dtype=np.float32)[:, None] * inverse[None, :]
        cosine, sine = np.cos(angles), np.sin(angles)
        table = np.zeros((3, count, D), np.float32)
        lo = half * 2 * quarter
        table[0, :, lo : lo + quarter] = cosine
        table[0, :, lo + quarter : lo + 2 * quarter] = cosine
        table[1, :, lo + quarter : lo + 2 * quarter] = sine
        table[2, :, lo : lo + quarter] = -sine
        return table

    rows = one(2048 // GRID_W, 0).reshape(3, 2048 // GRID_W, 1, D)
    cols = one(GRID_W, 1)
    return rows, cols


def rotate(n, c, s1, s2):
    return n * c + pltpu.roll(n, 32, 1) * s1 + pltpu.roll(n, 96, 1) * s2


def unrotate(n, c, s1, s2):
    return n * c - pltpu.roll(n, 32, 1) * s1 - pltpu.roll(n, 96, 1) * s2


def inv_rms(u):
    return lax.rsqrt(jnp.mean(u * u, axis=1, keepdims=True) + EPS)


def norm_back(grad, u, gain, c, s1, s2):
    r = inv_rms(u)
    t = unrotate(grad, c, s1, s2) * gain
    dot = jnp.sum(t * u, axis=1, keepdims=True)
    return r * t - u * (r * r * r * (1.0 / D) * dot)


def dot_nt(a, b):
    return lax.dot_general(a, b, (((1,), (1,)), ((), ())), preferred_element_type=F32)


def dot_nn(a, b):
    return lax.dot_general(a, b, (((1,), (0,)), ((), ())), preferred_element_type=F32)


def dot_tn(a, b):
    return lax.dot_general(a, b, (((0,), (0,)), ((), ())), preferred_element_type=F32)


def body(
    q, k_in, v, g, li, kw, vw, qg_in, kg_in, tr_in, tc_in,
    gq, gin, gwv, gwk,
    k, qg, kg, tr, tc, q_all, g_all, k_all, v_all, k_src, k_t, tab, qs, gs, m_scr, rl_scr, d_scr, s_all, dp_all, pb, ds,
    dq_out, dk_src, dv_in, dk_in, li_all, kw_s, vw_s, vs_all, ks_all,
    r1, st1, r2, go,
    loc, zs, zr, xs, xr, misc, dps, dpr, as_, ar, ts, trs,
):
    sp = lax.axis_index("sp")
    dp = lax.axis_index("dp")
    z, x = sp // NX, lax.rem(sp, NX)
    y, core = dp // 2, lax.rem(dp, 2)

    def remote(src, dst, ss, rs, **where):
        return pltpu.make_async_remote_copy(
            src_ref=src, dst_ref=dst, send_sem=ss, recv_sem=rs,
            device_id=where, device_id_type=pl.DeviceIdType.MESH,
        )

    def sent(ref, sem):
        remote(ref, ref, sem, sem, sp=sp).wait_send()

    def landed(ref, sem):
        remote(ref, ref, sem, sem, sp=sp).wait_recv()

    barrier = pltpu.get_barrier_semaphore()

    def greet_sp(o, _):
        pl.semaphore_signal(
            barrier, inc=1, device_id={"sp": lax.rem(sp + o, NSP)},
            device_id_type=pl.DeviceIdType.MESH,
        )
        return 0

    def greet_dp(o, _):
        pl.semaphore_signal(
            barrier, inc=1, device_id={"dp": lax.rem(dp + o, NDP)},
            device_id_type=pl.DeviceIdType.MESH,
        )
        return 0

    lax.fori_loop(1, NSP, greet_sp, 0)
    lax.fori_loop(1, NDP, greet_dp, 0)

    def cols(i, w):
        return pl.ds(pl.multiple_of(i * w, w), w)

    small = [
        pltpu.make_async_copy(src, dst, loc.at[7 + i])
        for i, (src, dst) in enumerate(
            ((k_in, k), (qg_in, qg), (kg_in, kg), (tr_in, tr), (tc_in, tc))
        )
    ]
    for c in small:
        c.start()
    own = [
        pltpu.make_async_copy(q.at[:, cols(z, 512)], q_all.at[z], loc.at[0]),
        pltpu.make_async_copy(g.at[:, cols(z, 512)], g_all.at[z], loc.at[1]),
        pltpu.make_async_copy(v.at[:, cols(z, D)], v_all.at[x, z], loc.at[2]),
        pltpu.make_async_copy(li.at[:, cols(dp, 512)], li_all.at[dp], loc.at[3]),
        pltpu.make_async_copy(kw, kw_s, loc.at[4]),
        pltpu.make_async_copy(vw, vw_s, loc.at[5]),
    ]
    for c in own:
        c.start()
    for c in small:
        c.wait()

    for zz in range(NZ):
        shard = NX * zz + x
        for kind in range(3):
            part = tc[kind]
            tab[zz, kind, 0:64] = part + tr[kind, 2 * shard]
            tab[zz, kind, 64:128] = part + tr[kind, 2 * shard + 1]

    for h in range(NZ):
        u = k[:, h * D : (h + 1) * D].astype(F32)
        n = u * inv_rms(u) * kg[...]
        k_src[h] = rotate(n, tab[z, 0], tab[z, 1], tab[z, 2]).astype(BF)
    k_all[x, z] = k_src[z]

    with jax.named_scope("s_barrier"):
        pl.semaphore_wait(barrier, NSP + NDP - 2)

    def z_copies(o, side, kinds):
        peer = lax.rem(z + o, NZ)
        slot = z if side == "send" else peer
        pairs = (
            (k_src.at[peer], k_all.at[x, slot]),
            (v.at[:, cols(peer, D)], v_all.at[x, slot]),
            (q.at[:, cols(peer, 512)], q_all.at[slot]),
            (g.at[:, cols(peer, 512)], g_all.at[slot]),
        )
        return [
            remote(*pairs[i], zs.at[i], zr.at[i // 2, slot], sp=peer * NX + x) for i in kinds
        ]

    order = (1, 3, 2)
    own[2].wait()
    for o in order:
        for c in z_copies(o, "send", (0, 1)):
            c.start()

    kv = (k_all, v_all)

    def rem4(i):
        return lax.rem(i + 4, 4)

    def x_copy(kind, chunk, zz, peer, ss, rs):
        at = kv[kind].at[chunk, zz]
        return remote(at, at, xs.at[ss], xr.at[rs], sp=z * NX + peer)

    def x_send(zz):
        x_copy(0, x, zz, rem4(x - 1), 0, zz).start()
        x_copy(1, x, zz, rem4(x + 1), 0, 4 + zz).start()
        x_copy(0, x, zz, rem4(x + 1), 0, 8).start()
        x_copy(1, x, zz, rem4(x - 1), 0, 8).start()

    x_send(z)
    for o in (1, 3):
        for c in z_copies(o, "send", (2, 3)):
            c.start()

    def li_copy(o, side):
        peer = lax.rem(dp + o, NDP)
        slot = dp if side == "send" else peer
        return remote(li.at[:, cols(peer, 512)], li_all.at[slot], misc.at[0], misc.at[1], dp=peer)

    def li_start(o, _):
        li_copy(o, "send").start()
        return 0

    lax.fori_loop(1, NDP, li_start, 0)

    def dq_copy(zz):
        return remote(dq_out.at[zz], gq.at[:, cols(z, 512)], misc.at[2], misc.at[3], sp=zz * NX + x)

    def prepare(o):
        zz = lax.rem(z + o, NZ)
        for h in range(4):
            rows = pl.ds(pl.multiple_of(o * 512 + h * T, T), T)
            u = q_all[zz, :, h * D : (h + 1) * D].astype(F32)
            n = u * inv_rms(u) * qg[...]
            qs[rows, :] = rotate(n, tab[zz, 0], tab[zz, 1], tab[zz, 2]).astype(BF)
            gs[rows, :] = g_all[zz, :, h * D : (h + 1) * D]

    def unit(xo, o):
        xx = lax.rem(x + xo, NX)
        qcols = pl.ds(pl.multiple_of(o * 512, 512), 512)
        qb, gb = qs[qcols, :], gs[qcols, :]
        for half in range(2):
            kc = k_all[xx, 2 * half : 2 * half + 2].reshape(256, D)
            vc = v_all[xx, 2 * half : 2 * half + 2].reshape(256, D)
            rows = pl.ds(pl.multiple_of(xx * 512 + half * 256, 256), 256)
            s = dot_nt(kc, qb)
            s_all[2 * o, rows, :] = s[:, :256]
            s_all[2 * o + 1, rows, :] = s[:, 256:]
            m_scr[:, qcols] = jnp.maximum(m_scr[:, qcols], jnp.max(s.reshape(32, 8, 512), axis=0))
            w = dot_nt(vc, gb)
            dp_all[2 * o, rows, :] = w[:, :256]
            dp_all[2 * o + 1, rows, :] = w[:, 256:]

    m_scr[...] = jnp.full((8, 2048), -jnp.inf, F32)
    own[0].wait()
    own[1].wait()
    def block_cols(i):
        return pl.ds(pl.multiple_of(i * 256, 256), 256)

    def exps(i, j, m, l8):
        at = slice(j * KC, (j + 1) * KC)
        e = jnp.exp2(s_all[i, at, :] * EXP2_SCALE - m)
        s_all[i, at, :] = e
        return l8 + jnp.sum(e.reshape(KC // 8, 8, 256), axis=0)

    def soft(i):
        m = jnp.max(m_scr[:, block_cols(i)], axis=0, keepdims=True) * EXP2_SCALE
        l8 = jnp.zeros((8, 256), F32)
        for j in range(2048 // KC):
            l8 = exps(i, j, m, l8)
        probs(i, l8)

    def whole(i):
        rows = pl.ds(pl.multiple_of(i * 256, 256), 256)
        qb, gb = qs[rows, :], gs[rows, :]
        m8 = jnp.full((8, 256), -jnp.inf, F32)
        for j in range(NX):
            s = dot_nt(k_all[j].reshape(512, D), qb)
            s_all[i, j * 512 : (j + 1) * 512, :] = s
            m8 = jnp.maximum(m8, jnp.max(s.reshape(64, 8, 256), axis=0))
        m = jnp.max(m8, axis=0, keepdims=True) * EXP2_SCALE
        l8 = jnp.zeros((8, 256), F32)
        for j in range(2 * NX):
            vb = v_all[j // 2, 2 * (j % 2) : 2 * (j % 2) + 2].reshape(256, D)
            dp_all[i, j * 256 : (j + 1) * 256, :] = dot_nt(vb, gb)
            for n in range(4):
                l8 = exps(i, 4 * j + n, m, l8)
        probs(i, l8)

    def probs(i, l8):
        here = block_cols(i)
        rl = 1.0 / jnp.sum(l8, axis=0, keepdims=True)
        rl_scr[:, here] = jnp.broadcast_to(rl, (8, 256))
        d8 = jnp.zeros((8, 256), F32)
        for j in range(2048 // KC):
            at = slice(j * KC, (j + 1) * KC)
            p_b = (s_all[i, at, :] * rl).astype(BF)
            pb[i, at, :] = p_b
            prod = p_b.astype(F32) * dp_all[i, at, :]
            d8 = d8 + jnp.sum(prod.reshape(KC // 8, 8, 256), axis=0)
        d_scr[:, here] = d8

    def scores(i):
        here = block_cols(i)
        delta = jnp.sum(d_scr[:, here], axis=0, keepdims=True)
        rl = rl_scr[0:1, here]
        for j in range(2048 // KC):
            at = slice(j * KC, (j + 1) * KC)
            ds[i, at, :] = ((s_all[i, at, :] * rl) * (dp_all[i, at, :] - delta)).astype(BF)

    prepare(0)
    with jax.named_scope("s_zkv"):
        for o in order:
            landed(k_src.at[0:2], zr.at[0, rem4(z + o)])
            x_send(rem4(z + o))
        for c in z_copies(2, "send", (2, 3)):
            c.start()
    with jax.named_scope("s_u0"):
        unit(0, 0)
    with jax.named_scope("s_u1"):
        for o in (0, 1, 3, 2):
            zz = rem4(z + o)
            landed(k_src.at[0], xr.at[zz])
            x_copy(0, rem4(x + 1), zz, rem4(x - 1), 1, 9).start()
            landed(k_src.at[0], xr.at[4 + zz])
            x_copy(1, rem4(x - 1), zz, rem4(x + 1), 1, 9).start()
        landed(k_all.at[0:2], xr.at[8])
        unit(1, 0)
        unit(3, 0)
        landed(k_all.at[0:2], xr.at[9])
        unit(2, 0)

    def block(i, _):
        soft(i)
        scores(i)
        return 0

    with jax.named_scope("s_b0"):
        lax.fori_loop(0, 2, block, 0)

    def whole_block(i, _):
        whole(i)
        scores(i)
        return 0

    def shard(i, _):
        o = 1 + 2 * i - 3 * (i // 2)
        with jax.named_scope("s_qw"):
            landed(q_all.at[0:2], zr.at[1, rem4(z + o)])
        prepare(o)
        lax.fori_loop(2 * o, 2 * o + 2, whole_block, 0)
        return 0

    with jax.named_scope("s_b1"):
        lax.fori_loop(0, 3, shard, 0)
    k_t[...] = k_all[...].reshape(NSP * T, D).T
    def grads_out(left, right, src, into, which):
        def step(t, _):
            xx = lax.rem(x + 1 + t, NX)
            at = pl.ds(pl.multiple_of(xx * 512, 512), 512)
            out = dot_nn(left[0, at, :], right[0:256, :])
            for j in range(1, 8):
                out = out + dot_nn(left[j, at, :], right[j * 256 : (j + 1) * 256, :])
            for zz in range(NZ):
                src(xx, zz)[...] = out[zz * T : (zz + 1) * T].astype(BF)
            for zz in range(NZ):
                peer = zz * NX + xx

                @pl.when(peer != sp)
                def _():
                    remote(
                        src(xx, zz), into.at[sp], dps.at[which], dpr.at[which], sp=peer
                    ).start()

            return 0

        lax.fori_loop(0, NX, step, 0)
        into[sp] = src(x, z)[...]

    def wait_grads(into, which):
        landed(into.at[0 : NSP - 1], dpr.at[which])

    def head_sum(into, h):
        total = into[NX * h].astype(F32)
        for xx in range(1, NX):
            total = total + into[NX * h + xx].astype(F32)
        return total

    def along_y(o, slot_y, rows, buf, which):
        peer = rem4(y + o)
        at = buf.at[2 * slot_y + core, rows]
        return remote(at, at, as_.at[which], ar.at[which, slot_y], dp=2 * peer + core)

    def cross(yy, buf, which):
        slot = 2 * yy + core
        return remote(
            buf.at[slot], buf.at[slot], as_.at[which], ar.at[which, 4], dp=2 * y + (1 - core)
        )

    def gather_start(buf, which):
        along_y(1, y, slice(0, T), buf, which).start()
        along_y(3, y, slice(0, T), buf, which).start()
        cross(y, buf, which).start()

    def gather_relay(buf, which):
        for o in (1, 3):
            yy = rem4(y + o)
            landed(buf.at[0], ar.at[which, yy])
            along_y(4 - o, yy, slice(0, 64) if o == 1 else slice(64, T), buf, which).start()
            cross(yy, buf, which).start()

    def gather_last(buf, which):
        yy = rem4(y + 2)
        landed(buf.at[0], ar.at[which, yy])
        cross(yy, buf, which).start()

    def gather_finish(buf, which):
        landed(buf.at[0:4], ar.at[which, 4])

    def gi_src(peer):
        return li_all.at[peer]

    outs = (gwv, gwk)

    def stage_copy(stage, which, half, o):
        along_x = (half == 0) == (stage != 1)
        me = x if along_x else z
        peer = rem4(me + o)
        wide = slice(half * 256, (half + 1) * 256)
        if stage == 0:
            src = pb.at[half, pl.ds(pl.multiple_of(which * 512 + peer * T, T), T)]
            dst = r1.at[which, half, me]
        elif stage == 1:
            src, dst = st1.at[which, half], r2.at[which, half, me]
        else:
            src, dst = go.at[which, half], outs[which].at[cols(me, T), wide]
        target = z * NX + peer if along_x else peer * NX + x
        return remote(src, dst, ts.at[stage], trs.at[stage, which, half], sp=target)

    def stage_start(stage, which, half):
        for o in (2, 1, 3):
            stage_copy(stage, which, half, o).start()

    def stage_wait(stage, which, half):
        landed(r1.at[which, half, 0:3], trs.at[stage, which, half])

    def own_part(which, half):
        return pltpu.make_async_copy(
            go.at[which, half],
            outs[which].at[cols(x if half == 0 else z, T), half * 256 : (half + 1) * 256],
            loc.at[12 + 2 * which + half],
        )

    def reduce_start(buf, which):
        out = dot_tn(li_all[...].reshape(NDP * T, 512), buf[...].reshape(NDP * T, 512))
        for half in range(2):
            pb[half, which * 512 : (which + 1) * 512, :] = out[:, half * 256 : (half + 1) * 256].astype(BF)
        for half in range(2):
            stage_start(0, which, half)

    def reduce_first(which):
        for half in range(2):
            me = x if half == 0 else z
            stage_wait(0, which, half)
            at = pl.ds(pl.multiple_of(which * 512 + me * T, T), T)
            total = pb[half, at].astype(F32)
            for o in order:
                total = total + r1[which, half, rem4(me + o)].astype(F32)
            st1[which, half] = total.astype(BF)
            stage_start(1, which, half)

    def reduce_second(which):
        for half in range(2):
            me = z if half == 0 else x
            stage_wait(1, which, half)
            total = st1[which, half].astype(F32)
            for o in order:
                total = total + r2[which, half, rem4(me + o)].astype(F32)
            go[which, half] = total.astype(BF)
            stage_start(2, which, half)
            own_part(which, half).start()

    with jax.named_scope("s_dk"):
        grads_out(ds, qs, lambda xx, zz: dk_src.at[xx, zz], dk_in, 1)

    def query_grads(i):
        off = i // 2
        zz = lax.rem(z + off, NZ)
        pair = lax.rem(i, 2)
        wide = pl.ds(pl.multiple_of(pair * 256, 256), 256)
        grad = dot_nn(k_t[...], ds[i]).T * SCALE
        both = q_all[zz, :, wide].astype(F32)
        outs = []
        for h in range(2):
            outs.append(
                norm_back(
                    grad[h * D : (h + 1) * D], both[:, h * D : (h + 1) * D], qg[...],
                    tab[zz, 0], tab[zz, 1], tab[zz, 2],
                ).astype(BF)
            )
        dq_out[zz, :, wide] = jnp.concatenate(outs, axis=1)

    def query_send(i):
        off = i // 2
        zz = lax.rem(z + off, NZ)
        pair = lax.rem(i, 2)

        if isinstance(i, int):
            if i == 1:
                pltpu.make_async_copy(dq_out.at[z], gq.at[:, cols(z, 512)], loc.at[6]).start()
            else:
                dq_copy(zz).start()
        else:

            @pl.when(pair == 1)
            def _():
                dq_copy(zz).start()

    def back(t, _):
        query_grads(t)

        @pl.when(t >= 4)
        def _():
            query_send(t)

        return 0

    with jax.named_scope("s_dq1"):
        lax.fori_loop(0, 4, back, 0)
    with jax.named_scope("s_dv"):
        grads_out(pb, gs, lambda xx, zz: g_all.at[xx, :, cols(zz, D)], dv_in, 0)
    query_send(1)
    query_send(3)
    with jax.named_scope("s_wdk"):
        wait_grads(dk_in, 1)
    pieces = []
    for h in range(NZ):
        u = k[:, h * D : (h + 1) * D].astype(F32)
        pieces.append(
            norm_back(head_sum(dk_in, h) * SCALE, u, kg[...], tab[z, 0], tab[z, 1], tab[z, 2]).astype(BF)
        )
    ks_all[dp] = jnp.concatenate(pieces, axis=1)
    gather_start(ks_all, 1)

    with jax.named_scope("s_dq2"):
        lax.fori_loop(4, 8, back, 0)
    with jax.named_scope("s_rlk"):
        gather_relay(ks_all, 1)
    with jax.named_scope("s_wdv"):
        wait_grads(dv_in, 0)
    vs_all[dp] = jnp.concatenate([head_sum(dv_in, h).astype(BF) for h in range(NZ)], axis=1)
    gather_start(vs_all, 0)
    own[3].wait()

    landed(li_all.at[0 : NDP - 1], misc.at[1])
    with jax.named_scope("s_gfk"):
        gather_last(ks_all, 1)
        gather_finish(ks_all, 1)
    with jax.named_scope("s_rsk"):
        reduce_start(ks_all, 1)
    with jax.named_scope("s_gfv"):
        gather_relay(vs_all, 0)
        gather_last(vs_all, 0)
        gather_finish(vs_all, 0)
    with jax.named_scope("s_rsv"):
        reduce_start(vs_all, 0)

    with jax.named_scope("s_rf1k"):
        reduce_first(1)

    own[4].wait()
    own[5].wait()

    def gi_copy(peer):
        return remote(gi_src(peer), gin.at[:, cols(dp, 512)], misc.at[4], misc.at[5], dp=peer)

    def grad_in(i, _):
        group = lax.rem(dp // 4 + 1 + i, 2)
        four = pl.ds(4 * group, 4)
        out = dot_nt(ks_all[four].reshape(512, 512), kw_s[...])
        out = out + dot_nt(vs_all[four].reshape(512, 512), vw_s[...])
        li_all[four] = out.astype(BF).reshape(4, T, 512)
        for j in range(4):
            peer = 4 * group + j

            @pl.when(peer != dp)
            def _():
                gi_copy(peer).start()

        return 0

    with jax.named_scope("s_gin"):
        lax.fori_loop(0, 2, grad_in, 0)
    pltpu.make_async_copy(gi_src(dp), gin.at[:, cols(dp, 512)], loc.at[16]).start()

    with jax.named_scope("s_rf1v"):
        reduce_first(0)
    with jax.named_scope("s_rf2"):
        reduce_second(1)
        reduce_second(0)
    sent(k_src.at[0:3], zs.at[0])
    sent(k_src.at[0:3], zs.at[1])
    sent(q_all.at[0:3], zs.at[2])
    sent(q_all.at[0:3], zs.at[3])
    sent(k_all, xs.at[0])
    sent(k_all.at[0:2], xs.at[1])
    sent(li_all.at[0 : NDP - 1], misc.at[0])
    sent(dq_out.at[0:3], misc.at[2])
    landed(dq_out.at[0:3], misc.at[3])
    for which, buf in ((0, vs_all), (1, ks_all)):
        sent(dv_in.at[0 : NSP - 1], dps.at[which])
        sent(buf.at[0 : NDP - 1], as_.at[which])
    pltpu.make_async_copy(dq_out.at[z], gq.at[:, cols(z, 512)], loc.at[6]).wait()
    pltpu.make_async_copy(gi_src(dp), gin.at[:, cols(dp, 512)], loc.at[16]).wait()
    with jax.named_scope("s_drdp"):
        sent(li_all.at[0 : NDP - 1], misc.at[4])
        landed(li_all.at[0 : NDP - 1], misc.at[5])
    with jax.named_scope("s_drsp"):
        for which in (1, 0):
            for half in range(2):
                stage_wait(2, which, half)
                own_part(which, half).wait()
        for stage in range(3):
            sent(r1.at[:, :, 0:3], ts.at[stage])


def finish(gq_in, gin_in, gwv_in, gwk_in, gq, gin, gwv, gwk, a, b, c, e, sem):
    ins, outs = [], []
    for i in range(4):
        at = slice(i * 32, (i + 1) * 32)
        rows = slice(i * T, (i + 1) * T)
        ins.append(
            [
                pltpu.make_async_copy(gwk_in.at[rows], c.at[0, rows], sem.at[0, i, 0]),
                pltpu.make_async_copy(gwv_in.at[rows], c.at[1, rows], sem.at[0, i, 1]),
                pltpu.make_async_copy(gin_in.at[at], b.at[at], sem.at[0, i, 2]),
                pltpu.make_async_copy(gq_in.at[at], a.at[at], sem.at[0, i, 3]),
            ]
        )
        outs.append(
            [
                pltpu.make_async_copy(e.at[0, rows], gwk.at[rows], sem.at[1, i, 0]),
                pltpu.make_async_copy(e.at[1, rows], gwv.at[rows], sem.at[1, i, 1]),
                pltpu.make_async_copy(b.at[at], gin.at[at], sem.at[1, i, 2]),
                pltpu.make_async_copy(a.at[at], gq.at[at], sem.at[1, i, 3]),
            ]
        )
    for group in ins:
        for copy in group:
            copy.start()
    for i in range(4):
        rows = slice(i * T, (i + 1) * T)
        for j in range(4):
            ins[i][j].wait()
            if j < 2:
                e[j, rows] = c[j, rows].astype(F32)
            outs[i][j].start()
    for group in outs:
        for copy in group:
            copy.wait()


def on_device(queries, keys, values, out_grad, layer_in, key_weight, value_weight, query_gain, key_gain):
    rows, cols = rope_tables()
    hbm = pl.BlockSpec(memory_space=pl.ANY)
    dma = pltpu.SemaphoreType.DMA
    V = pltpu.VMEM
    gq, gin, gwv, gwk = pl.pallas_call(
        body,
        out_shape=(
            jax.ShapeDtypeStruct((T, 2048), BF),
            jax.ShapeDtypeStruct((T, 4096), BF),
            jax.ShapeDtypeStruct((512, 512), BF),
            jax.ShapeDtypeStruct((512, 512), BF),
        ),
        in_specs=[hbm] * 11,
        out_specs=(hbm, hbm, hbm, hbm),
        scratch_shapes=[
            V((T, 512), BF),
            V((1, D), F32),
            V((1, D), F32),
            V(rows.shape, F32),
            V(cols.shape, F32),
            V((NZ, T, 512), BF),
            V((NZ, T, 512), BF),
            V((NX, NZ, T, D), BF),
            V((NX, NZ, T, D), BF),
            V((NZ, T, D), BF),
            V((D, 2048), BF),
            V((NZ, 3, T, D), F32),
            V((2048, D), BF),
            V((2048, D), BF),
            V((8, 2048), F32),
            V((8, 2048), F32),
            V((8, 2048), F32),
            V((8, 2048, 256), F32),
            V((8, 2048, 256), F32),
            V((8, 2048, 256), BF),
            V((8, 2048, 256), BF),
            V((NZ, T, 512), BF),
            V((NX, NZ, T, D), BF),
            V((NSP, T, D), BF),
            V((NSP, T, D), BF),
            V((NDP, T, 512), BF),
            V((512, 512), BF),
            V((512, 512), BF),
            V((NDP, T, 512), BF),
            V((NDP, T, 512), BF),
            V((2, 2, 4, T, 256), BF),
            V((2, 2, T, 256), BF),
            V((2, 2, 4, T, 256), BF),
            V((2, 2, T, 256), BF),
            dma((17,)),
            dma((4,)),
            dma((2, NZ)),
            dma((2,)),
            dma((10,)),
            dma((6,)),
            dma((2,)),
            dma((2,)),
            dma((2,)),
            dma((2, 5)),
            dma((3,)),
            dma((3, 2, 2)),
        ],
        compiler_params=pltpu.CompilerParams(
            collective_id=0, has_side_effects=True, vmem_limit_bytes=67043328
        ),
        name="step",
    )(
        queries[0], keys[0], values[0], out_grad[0], layer_in[0], key_weight, value_weight,
        query_gain.reshape(1, D), key_gain.reshape(1, D), jnp.asarray(rows), jnp.asarray(cols),
    )
    gq, gin, gwv, gwk = pl.pallas_call(
        finish,
        out_shape=(
            jax.ShapeDtypeStruct((T, 2048), BF),
            jax.ShapeDtypeStruct((T, 4096), BF),
            jax.ShapeDtypeStruct((512, 512), F32),
            jax.ShapeDtypeStruct((512, 512), F32),
        ),
        in_specs=[hbm] * 4,
        out_specs=(hbm,) * 4,
        scratch_shapes=[
            V((T, 2048), BF),
            V((T, 4096), BF),
            V((2, 512, 512), BF),
            V((2, 512, 512), F32),
            dma((2, 4, 4)),
        ],
        name="finish",
    )(gq, gin, gwv, gwk)
    return gq[None], gin[None], gwk, gwv


def solution(mesh):
    in_specs = (
        P("dp", "sp", None),
        P("dp", "sp", None),
        P("dp", "sp", None),
        P("dp", "sp", None),
        P("dp", "sp", None),
        P("dp", None),
        P("dp", None),
        P(),
        P(),
    )
    out_specs = (P("dp", "sp", None), P("dp", "sp", None), P("dp", None), P("dp", None))
    return jax.shard_map(
        on_device, mesh=mesh, in_specs=in_specs, out_specs=out_specs, check_vma=False
    )
```
